256 devices in a mesh: ep: 16 (over y, x), tp: 16 (over z, core).
Axes of the slice: x: 4, y: 4, z: 8, core: 2. Of those that a mesh axis runs over, the one named last changes fastest.
Arguments:
- mix_tokens: bfloat16 [4096, 4096], P('ep'), may hold values from -6 to 6
- mix_gain: float32 [4096], replicated, may hold values from 0.1 to 1.9
- value_weight: bfloat16 [4096, 2048], P(None, 'tp'), may hold values from -0.09375 to 0.09375
- inner_weight: bfloat16 [4096, 2048], P(None, 'tp'), may hold values from -0.09375 to 0.09375
- outer_weight: bfloat16 [4096, 2048], P(None, 'tp'), may hold values from -0.09375 to 0.09375
- conv_taps: float32 [3, 2048], P(None, 'tp'), may hold values from -3 to 3
- mix_weight: bfloat16 [2048, 4096], P('tp'), may hold values from -0.125 to 0.125
- moe_tokens: bfloat16 [4096, 4096], P('ep'), may hold values from -6 to 6
- moe_gain: float32 [4096], replicated, may hold values from 0.1 to 1.9
- router_group: bfloat16 [4096, 4], replicated, may hold values from -0.09375 to 0.09375
- router_expert: bfloat16 [4096, 16], replicated, may hold values from -0.09375 to 0.09375
- expert_routes: int32 [4096, 2], P('ep'), may hold values from 0 to 15, as said below
- gate_weight: bfloat16 [16, 4096, 2048], P('ep', None, 'tp'), may hold values from -0.09375 to 0.09375
- up_weight: bfloat16 [16, 4096, 2048], P('ep', None, 'tp'), may hold values from -0.09375 to 0.09375
- down_weight: bfloat16 [16, 2048, 4096], P('ep', 'tp'), may hold values from -0.5 to 0.5
Outputs:
- mixer_out: bfloat16 [4096, 4096], P(('ep', 'tp'))
- expert_out: bfloat16 [4096, 4096], P(('ep', 'tp'))
The draws below stay inside these ranges and needn't reach their ends.
Inputs may be any that keep to these rules, and one draw needn't show every extreme that they name: `expert_routes`: the two experts of a row are different and lie in one group of 4 consecutive expert numbers. In each aligned block of 16 rows no expert is named more than 4 times, and in every draw some experts are named exactly 4 times in every block.
All inputs are finite; a program needn't handle non-finite values.
Results may differ from the reference program's by a relative error of at most 0.0076.
Values may be sent and summed in bfloat16 or wider, within the bound.
No kernel may reach another device: no remote copies, remote signals or barrier semaphores. Data moves between devices by JAX's collectives and lax.ppermute only.
A program may use at most 128 MiB of HBM per device.

```python
import jax
import jax.numpy as jnp
from jax import lax

D = 4096
CONV_CH = 2048
TAPS = 3
FE = 2048
EXPERTS = 16
GROUPS = 4
TOPK = 2
MOE_SHARE = 16
EPG = 4
CAP = 4
MIX_TOKENS = 4096
MOE_TOKENS = 4096


def draw_expert_routes(key, part):
    blocks = MOE_TOKENS // MOE_SHARE
    half_share = MOE_SHARE // 2
    subkeys = jax.random.split(jax.random.fold_in(key, 7), 5)
    hot_group = jax.random.randint(subkeys[0], (), 0, GROUPS).astype(jnp.int32)
    others = (hot_group + 1 + jax.random.randint(subkeys[1], (blocks, MOE_SHARE - half_share), 0, GROUPS - 1)) % GROUPS
    labels = jnp.concatenate([jnp.full((blocks, half_share), hot_group, jnp.int32), others.astype(jnp.int32)], axis=1)
    scores = jax.random.randint(subkeys[2], (blocks, MOE_SHARE), 0, 1048576) * MOE_SHARE + jnp.arange(MOE_SHARE, dtype=jnp.int32)[None, :]
    ordering = jnp.argsort(scores, axis=1, stable=True)
    labels = jnp.take_along_axis(labels, ordering, axis=1)
    one_hot = (labels[:, :, None] == jnp.arange(GROUPS, dtype=jnp.int32)[None, None, :]).astype(jnp.int32)
    within = jnp.sum((jnp.cumsum(one_hot, axis=1) - one_hot) * one_hot, axis=2)
    offsets = jax.random.randint(subkeys[3], (blocks, GROUPS), 0, EPG)
    strides = jax.random.randint(subkeys[4], (blocks, GROUPS), 1, EPG)
    offset_tok = jnp.take_along_axis(offsets, labels, axis=1)
    stride_tok = jnp.take_along_axis(strides, labels, axis=1)
    first_pick = labels * EPG + (within + offset_tok) % EPG
    second_pick = labels * EPG + (within + offset_tok + stride_tok) % EPG
    return jnp.stack([first_pick, second_pick], axis=-1).reshape(blocks * MOE_SHARE, TOPK).astype(jnp.int32)


def levels(rng, shape, cuts, smallest, top_value):
    loudness = 1.0
    for dim, shards_of in cuts:
        draws = jax.random.uniform(jax.random.fold_in(jax.random.fold_in(rng, 6), dim), (shards_of,), jnp.float32, smallest / len(cuts), top_value / len(cuts))
        loudness = loudness * jnp.repeat(jnp.exp(draws), shape[dim] // shards_of).reshape((-1,) + (1,) * (len(shape) - 1 - dim))
    return loudness


def bell_draw(own_key, dims, deviation, limit, cuts=(), kind=jnp.bfloat16):
    values = deviation * jax.random.normal(own_key, dims, jnp.float32)
    if cuts:
        values = values * levels(own_key, dims, cuts, -0.22, 0.18)
    return jnp.clip(values, -limit, limit).astype(kind)


def setup_inputs(seed: int = 0) -> dict:
    seeds = jax.random.split(jax.random.key(seed), 16)
    return {
        "mix_tokens": bell_draw(seeds[0], (MIX_TOKENS, D), 1.0, 6.0, ((0, 16),)),
        "mix_gain": jnp.clip(1.0 + 0.18 * jax.random.normal(seeds[1], (D,), jnp.float32), 0.1, 1.9),
        "value_weight": bell_draw(seeds[2], (D, CONV_CH), D ** -0.5, 0.09375, ((1, 16),)),
        "inner_weight": bell_draw(seeds[3], (D, CONV_CH), D ** -0.5, 0.09375, ((1, 16),)),
        "outer_weight": bell_draw(seeds[4], (D, CONV_CH), D ** -0.5, 0.09375, ((1, 16),)),
        "conv_taps": bell_draw(seeds[5], (TAPS, CONV_CH), 0.6, 3.0, ((1, 16),), jnp.float32),
        "mix_weight": bell_draw(seeds[6], (CONV_CH, D), CONV_CH ** -0.5, 0.125, ((0, 16),)),
        "moe_tokens": bell_draw(seeds[7], (MOE_TOKENS, D), 1.0, 6.0, ((0, 16),)),
        "moe_gain": jnp.clip(1.0 + 0.18 * jax.random.normal(seeds[8], (D,), jnp.float32), 0.1, 1.9),
        "router_group": bell_draw(seeds[9], (D, GROUPS), D ** -0.5, 0.09375),
        "router_expert": bell_draw(seeds[10], (D, EXPERTS), D ** -0.5, 0.09375),
        "expert_routes": draw_expert_routes(jax.random.fold_in(seeds[15], 71), 0),
        "gate_weight": bell_draw(seeds[12], (EXPERTS, D, FE), D ** -0.5, 0.09375, ((0, 16), (2, 16))),
        "up_weight": bell_draw(seeds[13], (EXPERTS, D, FE), D ** -0.5, 0.09375, ((0, 16), (2, 16))),
        "down_weight": bell_draw(seeds[14], (EXPERTS, FE, D), (FE // 16) ** -0.5, 0.5, ((0, 16), (1, 16))),
    }


def rms_rows(inputs, gain_vec):
    values = inputs.astype(jnp.float32)
    inverse = lax.rsqrt(lax.optimization_barrier(jnp.mean(values * values, axis=-1, keepdims=True)) + 1e-06)
    return (values * inverse * gain_vec.astype(jnp.float32)).astype(jnp.bfloat16)

def route_weights(normed, routes, router_group, router_expert):
    group_logit = jnp.dot(normed, router_group, preferred_element_type=jnp.float32)
    expert_logit = jnp.dot(normed, router_expert, preferred_element_type=jnp.float32)
    group_exp = jnp.exp(group_logit)
    group_id = routes[:, 0] // EPG
    group_pick = (group_id[:, None] == jnp.arange(GROUPS, dtype=jnp.int32)[None, :]).astype(jnp.float32)
    group_gate = lax.optimization_barrier(jnp.sum(group_exp * group_pick, axis=1)) / lax.optimization_barrier(jnp.sum(group_exp, axis=1))
    expert_pick = (routes[:, :, None] == jnp.arange(EXPERTS, dtype=jnp.int32)[None, None, :]).astype(jnp.float32)
    chosen = jnp.exp(lax.optimization_barrier(jnp.sum(expert_logit[:, None, :] * expert_pick, axis=2)))
    return group_gate[:, None] * chosen / lax.optimization_barrier(jnp.sum(chosen, axis=1, keepdims=True))

def slot_ranks(routes):
    blocks = routes.shape[0] // MOE_SHARE
    entries = routes.reshape(blocks, MOE_SHARE * TOPK)
    one_hot = (entries[:, :, None] == jnp.arange(EXPERTS, dtype=jnp.int32)[None, None, :]).astype(jnp.int32)
    before = jnp.cumsum(one_hot, axis=1) - one_hot
    return lax.optimization_barrier(jnp.sum(before * one_hot, axis=2)).reshape(routes.shape)

def reference(mix_tokens, mix_gain, value_weight, inner_weight, outer_weight, conv_taps, mix_weight, moe_tokens, moe_gain, router_group, router_expert, expert_routes, gate_weight, up_weight, down_weight):
    normed = rms_rows(mix_tokens, mix_gain)
    value_proj = jnp.dot(normed, value_weight, preferred_element_type=jnp.float32)
    inner_proj = jnp.dot(normed, inner_weight, preferred_element_type=jnp.float32)
    outer_proj = jnp.dot(normed, outer_weight, preferred_element_type=jnp.float32)
    gated_in = lax.optimization_barrier((inner_proj * value_proj).astype(jnp.bfloat16)).astype(jnp.float32)
    seq_rows = gated_in.shape[0]
    padded = jnp.concatenate([jnp.zeros((TAPS - 1, gated_in.shape[1]), jnp.float32), gated_in], axis=0)
    tap_values = conv_taps.astype(jnp.float32)
    mixed_conv = tap_values[0] * padded[0:seq_rows]
    for tap_index in range(1, TAPS):
        mixed_conv = mixed_conv + tap_values[tap_index] * padded[tap_index:tap_index + seq_rows]
    conv_out = (outer_proj * mixed_conv).astype(jnp.bfloat16)
    mixer_out = jnp.dot(conv_out, mix_weight, preferred_element_type=jnp.float32).astype(jnp.bfloat16)
    moe_normed = rms_rows(moe_tokens, moe_gain)
    weights = route_weights(moe_normed, expert_routes, router_group, router_expert)
    ranks = slot_ranks(expert_routes)
    total_rows = moe_tokens.shape[0]
    block_id = jnp.arange(total_rows, dtype=jnp.int32) // MOE_SHARE
    position = (block_id[:, None] * CAP + ranks).astype(jnp.int32)
    per_expert = total_rows // MOE_SHARE * CAP
    token_id = jnp.broadcast_to(jnp.arange(total_rows, dtype=jnp.int32)[:, None], (total_rows, TOPK))
    slot_table = jnp.zeros((EXPERTS, per_expert), jnp.int32).at[expert_routes, position].set(token_id)

    def run_expert(operands):
        row_index, gate_w, up_w, down_w = operands
        picked_rows = moe_normed[row_index]
        gate_proj = jnp.dot(picked_rows, gate_w, preferred_element_type=jnp.float32)
        up_proj = jnp.dot(picked_rows, up_w, preferred_element_type=jnp.float32)
        hidden = (jax.nn.silu(gate_proj) * up_proj).astype(jnp.bfloat16)
        summed = jnp.dot(hidden, down_w, preferred_element_type=jnp.float32)
        return summed.astype(jnp.bfloat16)
    results = lax.map(run_expert, (slot_table, gate_weight, up_weight, down_weight))
    picked = results[expert_routes, position].astype(jnp.float32)
    expert_out = lax.optimization_barrier(jnp.sum(weights[:, :, None] * picked, axis=1)).astype(jnp.bfloat16)
    return (mixer_out, expert_out)
```

```python
import jax
import jax.numpy as jnp
from jax import lax
from jax.sharding import Mesh
from jax.sharding import PartitionSpec as P

TAPS = 3
EXPERTS = 16
GROUPS = 4
TOPK = 2
MOE_SHARE = 16
EPG = 4
CAP = 4

EP = ("y", "x")
TP = ("z", "core")
ALL = EP + TP


def rms_rows(inputs, gain_vec):
    values = inputs.astype(jnp.float32)
    inverse = lax.rsqrt(jnp.mean(values * values, axis=-1, keepdims=True) + 1e-06)
    return (values * inverse * gain_vec).astype(jnp.bfloat16)


def route_weights(normed, routes, router_group, router_expert):
    group_logit = jnp.dot(normed, router_group, preferred_element_type=jnp.float32)
    expert_logit = jnp.dot(normed, router_expert, preferred_element_type=jnp.float32)
    group_exp = jnp.exp(group_logit)
    group_id = routes[:, 0] // EPG
    group_pick = (group_id[:, None] == jnp.arange(GROUPS, dtype=jnp.int32)[None, :]).astype(
        jnp.float32
    )
    group_gate = jnp.sum(group_exp * group_pick, axis=1) / jnp.sum(group_exp, axis=1)
    expert_pick = (
        routes[:, :, None] == jnp.arange(EXPERTS, dtype=jnp.int32)[None, None, :]
    ).astype(jnp.float32)
    chosen = jnp.exp(jnp.sum(expert_logit[:, None, :] * expert_pick, axis=2))
    return group_gate[:, None] * chosen / jnp.sum(chosen, axis=1, keepdims=True)


def block_ranks(routes):
    blocks = routes.shape[0] // MOE_SHARE
    entries = routes.reshape(blocks, MOE_SHARE * TOPK)
    same = entries[:, :, None] == entries[:, None, :]
    place = jnp.arange(MOE_SHARE * TOPK, dtype=jnp.int32)
    earlier = place[None, :] < place[:, None]
    return jnp.sum((same & earlier[None]).astype(jnp.int32), axis=2).reshape(routes.shape)


def swap_cores(value):
    return lax.ppermute(value, "core", [(0, 1), (1, 0)])


def own_core_blocks(array, core):
    rows, width = array.shape
    blocks = rows // MOE_SHARE
    split = array.reshape(blocks // 2, 2, MOE_SHARE, width)
    return lax.dynamic_index_in_dim(split, core, 1, keepdims=False).reshape(rows // 2, width)


def both_cores(mine, theirs, axis):
    return jnp.concatenate([mine, theirs], axis=axis)


def mixer_partial(
    mix_tokens, mix_gain, value_weight, inner_weight, outer_weight, conv_taps, mix_weight2, core
):
    normed = rms_rows(mix_tokens, mix_gain)
    value_proj = jnp.dot(normed, value_weight, preferred_element_type=jnp.float32)
    inner_proj = jnp.dot(normed, inner_weight, preferred_element_type=jnp.float32)
    outer_proj = jnp.dot(normed, outer_weight, preferred_element_type=jnp.float32)
    gated_in = (inner_proj * value_proj).astype(jnp.bfloat16)
    count = lax.axis_size(EP)
    earlier = lax.ppermute(
        gated_in[gated_in.shape[0] - (TAPS - 1) :], EP, [(i, i + 1) for i in range(count - 1)]
    )
    padded = jnp.concatenate([earlier, gated_in], axis=0).astype(jnp.float32)
    seq_rows = gated_in.shape[0]
    mixed_conv = conv_taps[0] * padded[0:seq_rows]
    for tap_index in range(1, TAPS):
        mixed_conv = mixed_conv + conv_taps[tap_index] * padded[tap_index : tap_index + seq_rows]
    conv_out = (outer_proj * mixed_conv).astype(jnp.bfloat16)
    mine = own_core_blocks(conv_out, core)
    theirs = swap_cores(own_core_blocks(conv_out, 1 - core))
    channels = both_cores(mine, theirs, 1)
    return jnp.dot(channels, mix_weight2, preferred_element_type=jnp.float32).astype(jnp.bfloat16)


def local(
    mix_tokens,
    mix_gain,
    value_weight,
    inner_weight,
    outer_weight,
    conv_taps,
    mix_weight,
    moe_tokens,
    moe_gain,
    router_group,
    router_expert,
    expert_routes,
    gate_weight,
    up_weight,
    down_weight,
):
    z_index = lax.axis_index("z")
    core = lax.axis_index("core")
    zs = lax.axis_size("z")
    eps = lax.axis_size(EP)
    width = moe_tokens.shape[1]

    gate_up = jnp.concatenate([gate_weight[0], up_weight[0]], axis=1)
    gate_up2 = both_cores(gate_up, swap_cores(gate_up), 1)
    down2 = both_cores(down_weight[0], swap_cores(down_weight[0]), 0)
    mix_weight2 = both_cores(mix_weight, swap_cores(mix_weight), 0)

    half_routes = own_core_blocks(expert_routes, core)
    half_normed = rms_rows(own_core_blocks(moe_tokens, core), moe_gain)
    ranks = block_ranks(half_routes)
    block_id = jnp.arange(half_routes.shape[0], dtype=jnp.int32)[:, None] // MOE_SHARE
    slots = half_routes * (zs * CAP) + block_id * CAP + ranks
    targets = jnp.arange(EXPERTS * zs * CAP, dtype=jnp.int32)
    select = (slots[None, :, 0] == targets[:, None]) | (slots[None, :, 1] == targets[:, None])
    placed = jnp.dot(
        select.astype(jnp.bfloat16), half_normed, preferred_element_type=jnp.float32
    ).astype(jnp.bfloat16)
    arrived = lax.all_to_all(
        placed.reshape(EXPERTS, zs * CAP, width), EP, split_axis=0, concat_axis=0, tiled=True
    ).reshape(eps * zs * CAP, width)

    partial_mix = mixer_partial(
        mix_tokens, mix_gain, value_weight, inner_weight, outer_weight, conv_taps, mix_weight2, core
    )
    mixer_out = lax.psum_scatter(partial_mix, "z", scatter_dimension=0, tiled=True)
    arrived, partial_mix, gate_up2 = lax.optimization_barrier((arrived, partial_mix, gate_up2))

    both = jnp.dot(arrived, gate_up2, preferred_element_type=jnp.float32)
    units = gate_weight.shape[2]
    gate_proj = jnp.concatenate([both[:, 0:units], both[:, 2 * units : 3 * units]], axis=1)
    up_proj = jnp.concatenate([both[:, units : 2 * units], both[:, 3 * units :]], axis=1)
    hidden = (jax.nn.silu(gate_proj) * up_proj).astype(jnp.bfloat16)
    hidden = (
        hidden.reshape(eps, zs, CAP, 2 * units).transpose(1, 0, 2, 3).reshape(-1, 2 * units)
    )
    hidden, mixer_out, down2 = lax.optimization_barrier((hidden, mixer_out, down2))
    partial_value = jnp.dot(hidden, down2, preferred_element_type=jnp.float32).astype(jnp.bfloat16)
    results = lax.psum_scatter(partial_value, "z", scatter_dimension=0, tiled=True)
    returned = lax.all_to_all(
        results.reshape(eps, CAP, width), EP, split_axis=0, concat_axis=0, tiled=True
    ).reshape(EXPERTS * CAP, width)

    own_routes = lax.dynamic_slice_in_dim(half_routes, z_index * MOE_SHARE, MOE_SHARE, 0)
    own_normed = lax.dynamic_slice_in_dim(half_normed, z_index * MOE_SHARE, MOE_SHARE, 0)
    own_ranks = lax.dynamic_slice_in_dim(ranks, z_index * MOE_SHARE, MOE_SHARE, 0)
    weights = route_weights(own_normed, own_routes, router_group, router_expert)
    own_slots = own_routes * CAP + own_ranks
    picked = jnp.take(returned, own_slots, axis=0).astype(jnp.float32)
    expert_out = jnp.sum(weights[:, :, None] * picked, axis=1).astype(jnp.bfloat16)
    return (mixer_out, expert_out)


def solution(mesh):
    torus = Mesh(mesh.devices.reshape(4, 4, 8, 2), ALL)
    return jax.shard_map(
        local,
        mesh=torus,
        in_specs=(
            P(EP, None),
            P(),
            P(None, TP),
            P(None, TP),
            P(None, TP),
            P(None, TP),
            P(TP, None),
            P(EP, None),
            P(),
            P(),
            P(),
            P(EP, None),
            P(EP, None, TP),
            P(EP, None, TP),
            P(EP, TP, None),
        ),
        out_specs=(P(ALL, None), P(ALL, None)),
        check_vma=False,
    )
```

```python
import jax
import jax.numpy as jnp
from jax import lax
from jax.sharding import Mesh
from jax.sharding import PartitionSpec as P

TAPS = 3
EXPERTS = 16
GROUPS = 4
TOPK = 2
MOE_SHARE = 16
EPG = 4
CAP = 4

EP = ("y", "x")
TP = ("z", "core")
ALL = EP + TP


def rms_rows(inputs, gain_vec):
    values = inputs.astype(jnp.float32)
    inverse = lax.rsqrt(jnp.mean(values * values, axis=-1, keepdims=True) + 1e-06)
    return (values * inverse * gain_vec).astype(jnp.bfloat16)


def route_weights(normed, routes, router_group, router_expert):
    group_logit = jnp.dot(normed, router_group, preferred_element_type=jnp.float32)
    expert_logit = jnp.dot(normed, router_expert, preferred_element_type=jnp.float32)
    group_exp = jnp.exp(group_logit)
    group_id = routes[:, 0] // EPG
    group_pick = (group_id[:, None] == jnp.arange(GROUPS, dtype=jnp.int32)[None, :]).astype(
        jnp.float32
    )
    group_gate = jnp.sum(group_exp * group_pick, axis=1) / jnp.sum(group_exp, axis=1)
    expert_pick = (
        routes[:, :, None] == jnp.arange(EXPERTS, dtype=jnp.int32)[None, None, :]
    ).astype(jnp.float32)
    chosen = jnp.exp(jnp.sum(expert_logit[:, None, :] * expert_pick, axis=2))
    return group_gate[:, None] * chosen / jnp.sum(chosen, axis=1, keepdims=True)


def block_ranks(routes):
    blocks = routes.shape[0] // MOE_SHARE
    entries = routes.reshape(blocks, MOE_SHARE * TOPK)
    same = entries[:, :, None] == entries[:, None, :]
    place = jnp.arange(MOE_SHARE * TOPK, dtype=jnp.int32)
    earlier = place[None, :] < place[:, None]
    return jnp.sum((same & earlier[None]).astype(jnp.int32), axis=2).reshape(routes.shape)


def swap_cores(value):
    return lax.ppermute(value, "core", [(0, 1), (1, 0)])


def own_core_blocks(array, core):
    rows, width = array.shape
    blocks = rows // MOE_SHARE
    split = array.reshape(blocks // 2, 2, MOE_SHARE, width)
    return lax.dynamic_index_in_dim(split, core, 1, keepdims=False).reshape(rows // 2, width)


def both_cores(mine, theirs, axis):
    return jnp.concatenate([mine, theirs], axis=axis)


def mixer_channels(
    mix_tokens, before, mix_gain, weights, taps, core
):
    rows, width = mix_tokens.shape
    reach = TAPS - 1
    padded = jnp.concatenate([before, mix_tokens], axis=0)
    windows = [
        lax.dynamic_slice_in_dim(padded, (2 * block + core) * MOE_SHARE, MOE_SHARE + reach, 0)
        for block in range(rows // (2 * MOE_SHARE))
    ]
    normed = rms_rows(jnp.concatenate(windows, axis=0), mix_gain)
    value_proj, inner_proj, outer_proj = [
        jnp.concatenate(
            [jnp.dot(normed, part, preferred_element_type=jnp.float32) for part in pair], axis=1
        )
        for pair in weights
    ]
    channels = value_proj.shape[1]
    gated_in = (inner_proj * value_proj).astype(jnp.bfloat16).astype(jnp.float32)
    gated_in = gated_in.reshape(-1, MOE_SHARE + reach, channels)
    outer_proj = outer_proj.reshape(-1, MOE_SHARE + reach, channels)[:, reach:]
    mixed_conv = taps[0] * gated_in[:, 0:MOE_SHARE]
    for tap_index in range(1, TAPS):
        mixed_conv = mixed_conv + taps[tap_index] * gated_in[:, tap_index : tap_index + MOE_SHARE]
    return (outer_proj * mixed_conv).astype(jnp.bfloat16)


def swap_rows(array):
    return array.transpose(1, 0, 2)


def local(
    mix_tokens,
    mix_gain,
    value_weight,
    inner_weight,
    outer_weight,
    conv_taps,
    mix_weight,
    moe_tokens,
    moe_gain,
    router_group,
    router_expert,
    expert_routes,
    gate_weight,
    up_weight,
    down_weight,
):
    z_index = lax.axis_index("z")
    core = lax.axis_index("core")
    zs = lax.axis_size("z")
    eps = lax.axis_size(EP)
    width = moe_tokens.shape[1]
    units2 = 2 * gate_weight.shape[2]

    before = lax.ppermute(
        mix_tokens[mix_tokens.shape[0] - (TAPS - 1) :], EP, [(i, i + 1) for i in range(eps - 1)]
    )
    gate, up, down = gate_weight[0], up_weight[0], down_weight[0]
    swapped = [
        swap_cores(array)
        for array in (value_weight, inner_weight, outer_weight, mix_weight, gate, up, down)
    ]
    taps2 = both_cores(conv_taps, swap_cores(conv_taps), 1)
    down_mix = jnp.concatenate([down, swapped[6], mix_weight, swapped[3]], axis=0)
    gate_up = jnp.concatenate([gate, swapped[4], up, swapped[5]], axis=1)

    half_routes = own_core_blocks(expert_routes, core)
    half_normed = rms_rows(own_core_blocks(moe_tokens, core), moe_gain)
    ranks = block_ranks(half_routes)
    block_id = jnp.arange(half_routes.shape[0], dtype=jnp.int32)[:, None] // MOE_SHARE

    def dispatch(first, count, normed):
        position = (half_routes * count + ranks - first) * zs + block_id
        inside = (ranks >= first) & (ranks < first + count)
        position = jnp.where(inside, position, -1)
        targets = jnp.arange(EXPERTS * count * zs, dtype=jnp.int32)[:, None]
        select = (position[None, :, 0] == targets) | (position[None, :, 1] == targets)
        placed = jnp.dot(
            select.astype(jnp.bfloat16), normed, preferred_element_type=jnp.float32
        ).astype(jnp.bfloat16)
        return placed.reshape(EXPERTS, count * zs, width)

    def exchange(array):
        return lax.all_to_all(array, EP, split_axis=0, concat_axis=0, tiled=True)

    def expert_units(rows):
        both = jnp.dot(rows.reshape(-1, width), gate_up, preferred_element_type=jnp.float32)
        hidden = (jax.nn.silu(both[:, :units2]) * both[:, units2:]).astype(jnp.bfloat16)
        return swap_rows(hidden.reshape(-1, zs, units2))

    late = CAP - 1
    placed_first = dispatch(0, 1, half_normed)
    placed_first, half_late = lax.optimization_barrier((placed_first, half_normed))
    arrived_first = exchange(placed_first)
    arrived_late = exchange(dispatch(1, late, half_late))

    channels = mixer_channels(
        mix_tokens,
        before,
        mix_gain,
        (
            (value_weight, swapped[0]),
            (inner_weight, swapped[1]),
            (outer_weight, swapped[2]),
        ),
        taps2,
        core,
    )
    arrived_first, channels = lax.optimization_barrier((arrived_first, channels))

    first_units = expert_units(arrived_first)
    joint = jnp.concatenate(
        [
            jnp.concatenate([first_units, jnp.zeros_like(channels)], axis=2),
            jnp.concatenate([jnp.zeros_like(first_units), channels], axis=2),
        ],
        axis=1,
    )
    partial_first = jnp.dot(
        joint.reshape(-1, 2 * units2), down_mix, preferred_element_type=jnp.float32
    ).astype(jnp.bfloat16)
    arrived_late, _ = lax.optimization_barrier((arrived_late, partial_first))
    summed_first = lax.psum_scatter(partial_first, "z", scatter_dimension=0, tiled=True)
    mixer_out = summed_first[eps:]

    late_units = expert_units(arrived_late)
    partial_late = jnp.dot(
        late_units.reshape(-1, units2), down_mix[:units2], preferred_element_type=jnp.float32
    ).astype(jnp.bfloat16)
    summed_late = lax.psum_scatter(partial_late, "z", scatter_dimension=0, tiled=True)

    own_routes = lax.dynamic_slice_in_dim(half_routes, z_index * MOE_SHARE, MOE_SHARE, 0)
    own_normed = lax.dynamic_slice_in_dim(half_normed, z_index * MOE_SHARE, MOE_SHARE, 0)
    own_ranks = lax.dynamic_slice_in_dim(ranks, z_index * MOE_SHARE, MOE_SHARE, 0)
    weights = route_weights(own_normed, own_routes, router_group, router_expert)

    def combine(summed, first, count):
        returned = exchange(summed.reshape(eps, count * width // 128, 128)).reshape(-1, width)
        position = own_routes * count + own_ranks - first
        inside = (own_ranks >= first) & (own_ranks < first + count)
        position = jnp.where(inside, position, -1)
        targets = jnp.arange(EXPERTS * count, dtype=jnp.int32)
        spread = jnp.sum(
            jnp.where(position[:, :, None] == targets, weights[:, :, None], 0.0), axis=1
        )
        return jnp.dot(
            spread,
            returned.astype(jnp.float32),
            precision=lax.Precision.HIGHEST,
            preferred_element_type=jnp.float32,
        )

    expert_out = combine(summed_first[:eps], 0, 1) + combine(summed_late, 1, late)
    return (mixer_out, expert_out.astype(jnp.bfloat16))


def solution(mesh):
    torus = Mesh(mesh.devices.reshape(4, 4, 8, 2), ALL)
    return jax.shard_map(
        local,
        mesh=torus,
        in_specs=(
            P(EP, None),
            P(),
            P(None, TP),
            P(None, TP),
            P(None, TP),
            P(None, TP),
            P(TP, None),
            P(EP, None),
            P(),
            P(),
            P(),
            P(EP, None),
            P(EP, None, TP),
            P(EP, None, TP),
            P(EP, TP, None),
        ),
        out_specs=(P(ALL, None), P(ALL, None)),
        check_vma=False,
    )
```

```python
import functools

import jax
import jax.numpy as jnp
from jax import lax
from jax.experimental import pallas as pl
from jax.experimental.pallas import tpu as pltpu
from jax.sharding import Mesh
from jax.sharding import PartitionSpec as P


TAPS = 3
EXPERTS = 16
GROUPS = 4
TOPK = 2
MOE_SHARE = 16
EPG = 4
CAP = 4

EP = ("y", "x")
TP = ("z", "core")
ALL = EP + TP


def route_weights(normed, routes, router_group, router_expert):
    group_logit = jnp.dot(normed, router_group, preferred_element_type=jnp.float32)
    expert_logit = jnp.dot(normed, router_expert, preferred_element_type=jnp.float32)
    group_exp = jnp.exp(group_logit)
    group_id = routes[:, 0] // EPG
    group_pick = (group_id[:, None] == jnp.arange(GROUPS, dtype=jnp.int32)[None, :]).astype(
        jnp.float32
    )
    group_gate = jnp.sum(group_exp * group_pick, axis=1) / jnp.sum(group_exp, axis=1)
    expert_pick = (
        routes[:, :, None] == jnp.arange(EXPERTS, dtype=jnp.int32)[None, None, :]
    ).astype(jnp.float32)
    chosen = jnp.exp(jnp.sum(expert_logit[:, None, :] * expert_pick, axis=2))
    return group_gate[:, None] * chosen / jnp.sum(chosen, axis=1, keepdims=True)


def swap_cores(value):
    return lax.ppermute(value, "core", [(0, 1), (1, 0)])


def iota(shape, dim):
    return lax.broadcasted_iota(jnp.int32, shape, dim)


def select_matrix(mask):
    return jnp.where(mask, 1.0, 0.0).astype(jnp.bfloat16)


def product(left, right):
    return jnp.dot(left, right, preferred_element_type=jnp.float32)


def scaled_rows(rows, gain):
    values = rows.astype(jnp.float32)
    inverse = lax.rsqrt(jnp.mean(values * values, axis=-1, keepdims=True) + 1e-06)
    return (values * inverse * gain).astype(jnp.bfloat16)


def prep_kernel(zs, core_ref, tokens_ref, gain_ref, routes_ref, first_ref, late_ref, normed_ref, ranks_ref):
    share = MOE_SHARE
    rows = zs * share
    width = tokens_ref.shape[-1]
    normed_ref[...] = scaled_rows(tokens_ref[...].reshape(rows, width), gain_ref[...])
    token = iota((2 * rows, rows), 1)
    source = (token // share) * (2 * share) + core_ref[0] * share + token % share
    pick = select_matrix(iota((2 * rows, rows), 0) == source)
    routes = product(routes_ref[...].astype(jnp.float32).astype(jnp.bfloat16), pick).astype(jnp.int32)
    expert = iota((EXPERTS, rows), 0)
    named = [expert == routes[k : k + 1] for k in range(TOPK)]
    earlier, later = iota((rows, rows), 0), iota((rows, rows), 1)
    before = (earlier // share == later // share) & (earlier < later)
    counts = product(select_matrix(named[0] | named[1]), select_matrix(before))
    ranks = [
        jnp.sum(jnp.where(named[k], counts, 0.0), axis=0, keepdims=True).astype(jnp.int32)
        for k in range(TOPK)
    ]
    block = iota((1, rows), 1) // share
    late = CAP - 1
    slots_first = iota((EXPERTS * zs, rows), 0)
    slots_late = iota((EXPERTS * late * zs, rows), 0)
    in_first, in_late = [], []
    for k in range(TOPK):
        ranks_ref[k : k + 1, :] = ranks[k]
        chosen = routes[k : k + 1]
        spot = jnp.where(ranks[k] == 0, chosen * zs + block, -1)
        in_first.append(slots_first == spot)
        spot = jnp.where(ranks[k] > 0, (chosen * late + ranks[k] - 1) * zs + block, -1)
        in_late.append(slots_late == spot)
    select_first = select_matrix(in_first[0] | in_first[1])
    select_late = select_matrix(in_late[0] | in_late[1])
    step = 512

    @pl.loop(0, width // step)
    def _(index):
        columns = pl.ds(pl.multiple_of(index * step, step), step)
        piece = normed_ref[:, columns]
        first_ref[:, columns] = product(select_first, piece).astype(jnp.bfloat16)
        late_ref[:, columns] = product(select_late, piece).astype(jnp.bfloat16)


def prepare(core, tokens, gain, routes, zs):
    rows, width = tokens.shape
    half = rows // 2
    late = CAP - 1
    return pl.pallas_call(
        functools.partial(prep_kernel, zs),
        grid_spec=pltpu.PrefetchScalarGridSpec(
            num_scalar_prefetch=1,
            grid=(1,),
            in_specs=[
                pl.BlockSpec((zs, 1, MOE_SHARE, width), lambda i, c: (0, c[0], 0, 0)),
                pl.BlockSpec((1, width), lambda i, c: (0, 0)),
                pl.BlockSpec((TOPK, rows), lambda i, c: (0, 0)),
            ],
            out_specs=[
                pl.BlockSpec((EXPERTS * zs, width), lambda i, c: (0, 0)),
                pl.BlockSpec((EXPERTS * late * zs, width), lambda i, c: (0, 0)),
                pl.BlockSpec((half, width), lambda i, c: (0, 0)),
                pl.BlockSpec((TOPK, half), lambda i, c: (0, 0)),
            ],
        ),
        out_shape=[
            jax.ShapeDtypeStruct((EXPERTS * zs, width), jnp.bfloat16),
            jax.ShapeDtypeStruct((EXPERTS * late * zs, width), jnp.bfloat16),
            jax.ShapeDtypeStruct((half, width), jnp.bfloat16),
            jax.ShapeDtypeStruct((TOPK, half), jnp.int32),
        ],
        cost_estimate=pl.CostEstimate(
            flops=2 * EXPERTS * CAP * zs * half * width,
            bytes_accessed=2 * width * (rows + EXPERTS * CAP * zs),
            transcendentals=0,
        ),
        name="prepare",
    )(
        core,
        tokens.reshape(zs, 2, MOE_SHARE, width),
        gain.reshape(1, width),
        routes.T,
    )


def mixer_kernel(
    core_ref, tokens_ref, halo_ref, before_ref, gain_ref, taps_mine, taps_theirs, *refs
):
    weights, (out_ref, normed_ref, sums_ref) = refs[:6], refs[6:]
    step = pl.program_id(0)
    last = pl.num_programs(0) - 1
    rows, _ = out_ref.shape
    depth = weights[0].shape[0]
    width = tokens_ref.shape[-1]
    blocks, _, tail_rows, _ = halo_ref.shape
    halos = blocks * tail_rows
    total = normed_ref.shape[0]
    reach = TAPS - 1

    @pl.when(step == 0)
    def _():
        gain = gain_ref[...]
        normed_ref[0:rows, :] = scaled_rows(tokens_ref[...].reshape(rows, width), gain)
        normed_ref[rows : rows + halos, :] = scaled_rows(halo_ref[...].reshape(halos, width), gain)
        normed_ref[rows + halos :, :] = scaled_rows(before_ref[...], gain)
        sums_ref[...] = jnp.zeros_like(sums_ref)

    piece = normed_ref[:, pl.ds(pl.multiple_of(step * depth, depth), depth)]
    for index in range(6):
        sums_ref[index] += product(piece, weights[index][...])

    @pl.when(step == last)
    def _():
        def pair(index):
            return jnp.concatenate([sums_ref[index], sums_ref[index + 1]], axis=1)

        gated = (pair(2) * pair(0)).astype(jnp.bfloat16)
        row, source = iota((rows, total), 0), iota((rows, total), 1)
        place = row % MOE_SHARE
        ahead = row // MOE_SHARE + core_ref[0]
        tail = jnp.where(ahead == 0, total, rows + ahead * tail_rows)
        taps = jnp.concatenate([taps_mine[...], taps_theirs[...]], axis=1)
        mixed = None
        for tap in range(TAPS):
            back = reach - tap
            wanted = jnp.where(place >= back, row, tail + place) - back
            shifted = product(select_matrix(source == wanted), gated)
            term = taps[tap : tap + 1] * shifted
            mixed = term if mixed is None else mixed + term
        out_ref[...] = (pair(4)[0:rows] * mixed).astype(jnp.bfloat16)


def mixer_channels(core, tokens, before, gain, taps, weights, zs):
    rows, width = tokens.shape
    half = rows // 2
    channels = weights[0].shape[1]
    depth = 512
    tail_rows = MOE_SHARE // 2
    total = half + zs * tail_rows + before.shape[0]
    fixed = lambda i, c: (0, 0)
    split = tokens.reshape(zs, 2, MOE_SHARE, width)
    return pl.pallas_call(
        mixer_kernel,
        grid_spec=pltpu.PrefetchScalarGridSpec(
            num_scalar_prefetch=1,
            grid=(width // depth,),
            in_specs=[
                pl.BlockSpec((zs, 1, MOE_SHARE, width), lambda i, c: (0, c[0], 0, 0)),
                pl.BlockSpec((zs, 1, tail_rows, width), lambda i, c: (0, 1 - c[0], 1, 0)),
                pl.BlockSpec(before.shape, fixed),
                pl.BlockSpec((1, width), fixed),
                pl.BlockSpec((TAPS, channels), fixed),
                pl.BlockSpec((TAPS, channels), fixed),
            ]
            + [pl.BlockSpec((depth, channels), lambda i, c: (i, 0))] * 6,
            out_specs=pl.BlockSpec((half, 2 * channels), fixed),
            scratch_shapes=[
                pltpu.VMEM((total, width), jnp.bfloat16),
                pltpu.VMEM((6, total, channels), jnp.float32),
            ],
        ),
        out_shape=jax.ShapeDtypeStruct((half, 2 * channels), jnp.bfloat16),
        cost_estimate=pl.CostEstimate(
            flops=2 * (total) * width * 6 * channels,
            bytes_accessed=2 * width * (total + 6 * channels),
            transcendentals=0,
        ),
        name="mixer",
    )(core, split, split, before, gain.reshape(1, width), *taps, *weights)


def expert_kernel(zs, steps, joined, rows_ref, g0, g1, u0, u1, d0, d1, *refs):
    if joined:
        channels_ref, m0, m1, out_ref, sums_ref, units_ref, mixed_ref = refs
    else:
        out_ref, sums_ref, units_ref = refs
    step = pl.program_id(0)
    count = rows_ref.shape[0]
    given = out_ref.shape[0]
    half = g0.shape[1]

    @pl.when(step == 0)
    def _():
        sums_ref[...] = jnp.zeros_like(sums_ref)

    @pl.when(step < steps)
    def _():
        for index, weight in enumerate((g0, g1, u0, u1)):
            sums_ref[index] += product(rows_ref[...], weight[...])

    @pl.when(step == steps - 1)
    def _():
        target, source = iota((given, count), 0), iota((given, count), 1)
        order = select_matrix(target == (source % zs) * (given // zs) + source // zs)
        for index in range(2):
            gate, up = sums_ref[index], sums_ref[index + 2]
            hidden = (gate * jax.nn.sigmoid(gate) * up).astype(jnp.bfloat16)
            units_ref[:, index * half : (index + 1) * half] = product(order, hidden).astype(
                jnp.bfloat16
            )
        if joined:
            rows = channels_ref.shape[0]
            target, source = iota((given, rows), 0), iota((given, rows), 1)
            place = (source // MOE_SHARE + 1) * (given // zs) - MOE_SHARE + source % MOE_SHARE
            mixed_ref[...] = product(
                select_matrix(target == place), channels_ref[...]
            ).astype(jnp.bfloat16)

    @pl.when(step >= steps)
    def _():
        total = product(units_ref[:, :half], d0[...]) + product(units_ref[:, half:], d1[...])
        if joined:
            total = total + (
                product(mixed_ref[:, :half], m0[...]) + product(mixed_ref[:, half:], m1[...])
            )
        out_ref[...] = total.astype(jnp.bfloat16)


def expert_partial(rows, weights, downs, zs, channels=None, mixes=()):
    count, width = rows.shape
    half = weights[0].shape[1]
    depth = 512
    steps = width // depth
    joined = channels is not None
    given = count + (channels.shape[0] if joined else 0)
    early = lambda i: jnp.minimum(i, steps - 1)
    after = lambda i: jnp.maximum(i - steps, 0)
    in_specs = [pl.BlockSpec((count, depth), lambda i: (0, early(i)))]
    in_specs += [pl.BlockSpec((depth, half), lambda i: (early(i), 0))] * 4
    in_specs += [pl.BlockSpec((half, depth), lambda i: (0, after(i)))] * 2
    scratch = [
        pltpu.VMEM((4, count, half), jnp.float32),
        pltpu.VMEM((given, 2 * half), jnp.bfloat16),
    ]
    operands = (rows, *weights, *downs)
    if joined:
        in_specs += [pl.BlockSpec(channels.shape, lambda i: (0, 0))]
        in_specs += [pl.BlockSpec((half, depth), lambda i: (0, after(i)))] * 2
        scratch += [pltpu.VMEM((given, 2 * half), jnp.bfloat16)]
        operands += (channels, *mixes)
    return pl.pallas_call(
        functools.partial(expert_kernel, zs, steps, joined),
        grid=(2 * steps,),
        in_specs=in_specs,
        out_specs=pl.BlockSpec((given, depth), lambda i: (0, after(i))),
        scratch_shapes=scratch,
        out_shape=jax.ShapeDtypeStruct((given, width), jnp.bfloat16),
        cost_estimate=pl.CostEstimate(
            flops=2 * width * half * (4 * count + 2 * given),
            bytes_accessed=2 * width * (count + given + 6 * half),
            transcendentals=2 * count * half,
        ),
        name="experts_joined" if joined else "experts",
    )(*operands)


def layer(
    mix_tokens,
    mix_gain,
    value_weight,
    inner_weight,
    outer_weight,
    conv_taps,
    mix_weight,
    moe_tokens,
    moe_gain,
    router_group,
    router_expert,
    expert_routes,
    gate_weight,
    up_weight,
    down_weight,
):
    z_index = lax.axis_index("z")
    core = lax.axis_index("core")
    zs = lax.axis_size("z")
    eps = lax.axis_size(EP)
    width = moe_tokens.shape[1]
    core_ref = core.reshape(1).astype(jnp.int32)

    before = lax.ppermute(
        mix_tokens[mix_tokens.shape[0] - MOE_SHARE :], EP, [(i, i + 1) for i in range(eps - 1)]
    )
    gate, up, down = gate_weight[0], up_weight[0], down_weight[0]

    placed_first, placed_late, half_normed, half_ranks = prepare(
        core_ref, moe_tokens, moe_gain, expert_routes, zs
    )

    def exchange(array):
        return lax.all_to_all(array, EP, split_axis=0, concat_axis=0, tiled=True)

    late = CAP - 1
    arrived_first = exchange(placed_first.reshape(EXPERTS, zs, width))
    arrived_late = exchange(placed_late.reshape(EXPERTS, late * zs, width))

    taps = (conv_taps, swap_cores(conv_taps))
    projections = (
        value_weight,
        swap_cores(value_weight),
        inner_weight,
        swap_cores(inner_weight),
        outer_weight,
        swap_cores(outer_weight),
    )
    channels = mixer_channels(core_ref, mix_tokens, before, mix_gain, taps, projections, zs)
    arrived_first, channels = lax.optimization_barrier((arrived_first, channels))

    weights = (gate, swap_cores(gate), up, swap_cores(up))
    downs = (down, swap_cores(down))
    mixes = (mix_weight, swap_cores(mix_weight))
    partial_first = expert_partial(
        arrived_first.reshape(-1, width), weights, downs, zs, channels, mixes
    )
    arrived_late, _ = lax.optimization_barrier((arrived_late, partial_first))
    summed_first = lax.psum_scatter(partial_first, "z", scatter_dimension=0, tiled=True)
    mixer_out = summed_first[eps:]

    partial_late = expert_partial(arrived_late.reshape(-1, width), weights, downs, zs)
    summed_late = lax.psum_scatter(partial_late, "z", scatter_dimension=0, tiled=True)

    own_routes = lax.dynamic_slice_in_dim(
        expert_routes, (2 * z_index + core) * MOE_SHARE, MOE_SHARE, 0
    )
    own_normed = lax.dynamic_slice_in_dim(half_normed, z_index * MOE_SHARE, MOE_SHARE, 0)
    own_ranks = lax.dynamic_slice_in_dim(half_ranks, z_index * MOE_SHARE, MOE_SHARE, 1).T
    token_weights = route_weights(own_normed, own_routes, router_group, router_expert)

    def combine(summed, first, count):
        returned = exchange(summed.reshape(eps, count * width // 128, 128)).reshape(-1, width)
        position = own_routes * count + own_ranks - first
        inside = (own_ranks >= first) & (own_ranks < first + count)
        position = jnp.where(inside, position, -1)
        targets = jnp.arange(EXPERTS * count, dtype=jnp.int32)
        spread = jnp.sum(
            jnp.where(position[:, :, None] == targets, token_weights[:, :, None], 0.0), axis=1
        )
        return jnp.dot(
            spread,
            returned.astype(jnp.float32),
            precision=lax.Precision.HIGHEST,
            preferred_element_type=jnp.float32,
        )

    expert_out = combine(summed_first[:eps], 0, 1) + combine(summed_late, 1, late)
    return (mixer_out, expert_out.astype(jnp.bfloat16))


def solution(mesh):
    torus = Mesh(mesh.devices.reshape(4, 4, 8, 2), ALL)
    return jax.shard_map(
        layer,
        mesh=torus,
        in_specs=(
            P(EP, None),
            P(),
            P(None, TP),
            P(None, TP),
            P(None, TP),
            P(None, TP),
            P(TP, None),
            P(EP, None),
            P(),
            P(),
            P(),
            P(EP, None),
            P(EP, None, TP),
            P(EP, None, TP),
            P(EP, TP, None),
        ),
        out_specs=(P(ALL, None), P(ALL, None)),
        check_vma=False,
    )
```

```python
import functools

import jax
import jax.numpy as jnp
from jax import lax
from jax.experimental import pallas as pl
from jax.experimental.pallas import tpu as pltpu
from jax.sharding import Mesh
from jax.sharding import PartitionSpec as P


TAPS = 3
EXPERTS = 16
GROUPS = 4
TOPK = 2
MOE_SHARE = 16
EPG = 4
CAP = 4


EP = ("y", "x")
TP = ("z", "core")
ALL = EP + TP


def route_weights(normed, routes, router_group, router_expert):
    group_logit = jnp.dot(normed, router_group, preferred_element_type=jnp.float32)
    expert_logit = jnp.dot(normed, router_expert, preferred_element_type=jnp.float32)
    group_exp = jnp.exp(group_logit)
    group_id = routes[:, 0] // EPG
    group_pick = (group_id[:, None] == jnp.arange(GROUPS, dtype=jnp.int32)[None, :]).astype(
        jnp.float32
    )
    group_gate = jnp.sum(group_exp * group_pick, axis=1) / jnp.sum(group_exp, axis=1)
    expert_pick = (
        routes[:, :, None] == jnp.arange(EXPERTS, dtype=jnp.int32)[None, None, :]
    ).astype(jnp.float32)
    chosen = jnp.exp(jnp.sum(expert_logit[:, None, :] * expert_pick, axis=2))
    return group_gate[:, None] * chosen / jnp.sum(chosen, axis=1, keepdims=True)


def swap_cores(value):
    return lax.ppermute(value, "core", [(0, 1), (1, 0)])


def iota(shape, dim):
    return lax.broadcasted_iota(jnp.int32, shape, dim)


def select_matrix(mask):
    return jnp.where(mask, 1.0, 0.0).astype(jnp.bfloat16)


def product(left, right):
    return jnp.dot(left, right, preferred_element_type=jnp.float32)


def scaled_rows(rows, gain):
    values = rows.astype(jnp.float32)
    inverse = lax.rsqrt(jnp.mean(values * values, axis=-1, keepdims=True) + 1e-06)
    return (values * inverse * gain).astype(jnp.bfloat16)


def prep_kernel(zs, core_ref, tokens_ref, gain_ref, routes_ref, placed_ref, normed_ref, ranks_ref):
    share = MOE_SHARE
    rows = zs * share
    width = tokens_ref.shape[-1]
    normed_ref[...] = scaled_rows(tokens_ref[...].reshape(rows, width), gain_ref[...])
    token = iota((2 * rows, rows), 1)
    source = (token // share) * (2 * share) + core_ref[0] * share + token % share
    pick = select_matrix(iota((2 * rows, rows), 0) == source)
    routes = product(routes_ref[...].astype(jnp.float32).astype(jnp.bfloat16), pick).astype(jnp.int32)
    expert = iota((EXPERTS, rows), 0)
    named = [expert == routes[k : k + 1] for k in range(TOPK)]
    earlier, later = iota((rows, rows), 0), iota((rows, rows), 1)
    before = (earlier // share == later // share) & (earlier < later)
    counts = product(select_matrix(named[0] | named[1]), select_matrix(before))
    ranks = [
        jnp.sum(jnp.where(named[k], counts, 0.0), axis=0, keepdims=True).astype(jnp.int32)
        for k in range(TOPK)
    ]
    block = iota((1, rows), 1) // share
    slots = iota((EXPERTS * CAP * zs, rows), 0)
    inside = []
    for k in range(TOPK):
        ranks_ref[k : k + 1, :] = ranks[k]
        inside.append(slots == (routes[k : k + 1] * CAP + ranks[k]) * zs + block)
    select = select_matrix(inside[0] | inside[1])
    step = 512

    @pl.loop(0, width // step)
    def _(index):
        columns = pl.ds(pl.multiple_of(index * step, step), step)
        placed_ref[:, columns] = product(select, normed_ref[:, columns]).astype(jnp.bfloat16)


def prepare(core, tokens, gain, routes, zs):
    rows, width = tokens.shape
    half = rows // 2
    return pl.pallas_call(
        functools.partial(prep_kernel, zs),
        grid_spec=pltpu.PrefetchScalarGridSpec(
            num_scalar_prefetch=1,
            grid=(1,),
            in_specs=[
                pl.BlockSpec((zs, 1, MOE_SHARE, width), lambda i, c: (0, c[0], 0, 0)),
                pl.BlockSpec((1, width), lambda i, c: (0, 0)),
                pl.BlockSpec((TOPK, rows), lambda i, c: (0, 0)),
            ],
            out_specs=[
                pl.BlockSpec((EXPERTS * CAP * zs, width), lambda i, c: (0, 0)),
                pl.BlockSpec((half, width), lambda i, c: (0, 0)),
                pl.BlockSpec((TOPK, half), lambda i, c: (0, 0)),
            ],
        ),
        out_shape=[
            jax.ShapeDtypeStruct((EXPERTS * CAP * zs, width), jnp.bfloat16),
            jax.ShapeDtypeStruct((half, width), jnp.bfloat16),
            jax.ShapeDtypeStruct((TOPK, half), jnp.int32),
        ],
        cost_estimate=pl.CostEstimate(
            flops=2 * EXPERTS * CAP * zs * half * width,
            bytes_accessed=2 * width * (rows + EXPERTS * CAP * zs),
            transcendentals=0,
        ),
        name="prepare",
    )(
        core,
        tokens.reshape(zs, 2, MOE_SHARE, width),
        gain.reshape(1, width),
        routes.T,
    )


def mixer_kernel(
    steps, core_ref, tokens_ref, halo_ref, before_ref, gain_ref, taps_mine, taps_theirs, *refs
):
    weights, (m0, m1, out_ref, normed_ref, sums_ref, channels_ref) = refs[:6], refs[6:]
    step = pl.program_id(0)
    rows = out_ref.shape[0]
    depth, half = weights[0].shape
    width = tokens_ref.shape[-1]
    blocks, _, tail_rows, _ = halo_ref.shape
    halos = blocks * tail_rows
    total = normed_ref.shape[0]
    reach = TAPS - 1

    @pl.when(step == 0)
    def _():
        gain = gain_ref[...]
        normed_ref[0:rows, :] = scaled_rows(tokens_ref[...].reshape(rows, width), gain)
        normed_ref[rows : rows + halos, :] = scaled_rows(halo_ref[...].reshape(halos, width), gain)
        normed_ref[rows + halos :, :] = scaled_rows(before_ref[...], gain)
        sums_ref[...] = jnp.zeros_like(sums_ref)

    @pl.when(step < steps)
    def _():
        piece = normed_ref[:, pl.ds(pl.multiple_of(step * depth, depth), depth)]
        joint = jnp.concatenate([weight[...] for weight in weights], axis=1)
        sums_ref[...] += product(piece, joint)

    @pl.when(step == steps - 1)
    def _():
        def pair(index):
            return sums_ref[:, 2 * index * half : 2 * (index + 1) * half]

        gated = (pair(1) * pair(0)).astype(jnp.bfloat16)
        row, source = iota((rows, total), 0), iota((rows, total), 1)
        place = row % MOE_SHARE
        ahead = row // MOE_SHARE + core_ref[0]
        tail = jnp.where(ahead == 0, total, rows + ahead * tail_rows)
        taps = jnp.concatenate([taps_mine[...], taps_theirs[...]], axis=1)
        mixed = None
        for tap in range(TAPS):
            back = reach - tap
            wanted = jnp.where(place >= back, row, tail + place) - back
            shifted = product(select_matrix(source == wanted), gated)
            term = taps[tap : tap + 1] * shifted
            mixed = term if mixed is None else mixed + term
        channels_ref[...] = (pair(2)[0:rows] * mixed).astype(jnp.bfloat16)

    @pl.when(step >= steps)
    def _():
        joint = jnp.concatenate([m0[...], m1[...]], axis=0)
        out_ref[...] = product(channels_ref[...], joint).astype(jnp.bfloat16)


def mixer_partial(core, tokens, before, gain, taps, weights, mixes, zs):
    rows, width = tokens.shape
    half = rows // 2
    channels = weights[0].shape[1]
    depth = 1024
    steps = width // depth
    tail_rows = MOE_SHARE // 2
    total = half + zs * tail_rows + before.shape[0]
    fixed = lambda i, c: (0, 0)
    after = lambda i, c: (0, jnp.maximum(i - steps, 0))
    split = tokens.reshape(zs, 2, MOE_SHARE, width)
    return pl.pallas_call(
        functools.partial(mixer_kernel, steps),
        grid_spec=pltpu.PrefetchScalarGridSpec(
            num_scalar_prefetch=1,
            grid=(2 * steps,),
            in_specs=[
                pl.BlockSpec((zs, 1, MOE_SHARE, width), lambda i, c: (0, c[0], 0, 0)),
                pl.BlockSpec((zs, 1, tail_rows, width), lambda i, c: (0, 1 - c[0], 1, 0)),
                pl.BlockSpec(before.shape, fixed),
                pl.BlockSpec((1, width), fixed),
                pl.BlockSpec((TAPS, channels), fixed),
                pl.BlockSpec((TAPS, channels), fixed),
            ]
            + [pl.BlockSpec((depth, channels), lambda i, c: (jnp.minimum(i, steps - 1), 0))] * 6
            + [pl.BlockSpec((channels, depth), after)] * 2,
            out_specs=pl.BlockSpec((half, depth), after),
            scratch_shapes=[
                pltpu.VMEM((total, width), jnp.bfloat16),
                pltpu.VMEM((total, 6 * channels), jnp.float32),
                pltpu.VMEM((half, 2 * channels), jnp.bfloat16),
            ],
        ),
        out_shape=jax.ShapeDtypeStruct((half, width), jnp.bfloat16),
        cost_estimate=pl.CostEstimate(
            flops=2 * width * channels * (6 * total + 2 * half),
            bytes_accessed=2 * width * (total + half + 8 * channels),
            transcendentals=0,
        ),
        name="mixer",
    )(core, split, split, before, gain.reshape(1, width), *taps, *weights, *mixes)


def expert_kernel(zs, steps, rows_ref, g0, g1, u0, u1, d0, d1, out_ref, sums_ref, units_ref):
    step = pl.program_id(0)
    count = rows_ref.shape[0]
    units = 2 * g0.shape[1]

    @pl.when(step == 0)
    def _():
        sums_ref[...] = jnp.zeros_like(sums_ref)

    @pl.when(step < steps)
    def _():
        joint = jnp.concatenate([g0[...], g1[...], u0[...], u1[...]], axis=1)
        sums_ref[...] += product(rows_ref[...], joint)

    @pl.when(step == steps - 1)
    def _():
        target, source = iota((count, count), 0), iota((count, count), 1)
        order = select_matrix(target == (source % zs) * (count // zs) + source // zs)
        gate, up = sums_ref[:, :units], sums_ref[:, units:]
        hidden = (gate * jax.nn.sigmoid(gate) * up).astype(jnp.bfloat16)
        units_ref[...] = product(order, hidden).astype(jnp.bfloat16)

    @pl.when(step >= steps)
    def _():
        joint = jnp.concatenate([d0[...], d1[...]], axis=0)
        out_ref[...] = product(units_ref[...], joint).astype(jnp.bfloat16)


def expert_partial(rows, weights, downs, zs):
    count, width = rows.shape
    half = weights[0].shape[1]
    depth = 1024
    steps = width // depth
    early = lambda i: jnp.minimum(i, steps - 1)
    after = lambda i: jnp.maximum(i - steps, 0)
    return pl.pallas_call(
        functools.partial(expert_kernel, zs, steps),
        grid=(2 * steps,),
        in_specs=[pl.BlockSpec((count, depth), lambda i: (0, early(i)))]
        + [pl.BlockSpec((depth, half), lambda i: (early(i), 0))] * 4
        + [pl.BlockSpec((half, depth), lambda i: (0, after(i)))] * 2,
        out_specs=pl.BlockSpec((count, depth), lambda i: (0, after(i))),
        scratch_shapes=[
            pltpu.VMEM((count, 4 * half), jnp.float32),
            pltpu.VMEM((count, 2 * half), jnp.bfloat16),
        ],
        out_shape=jax.ShapeDtypeStruct((count, width), jnp.bfloat16),
        cost_estimate=pl.CostEstimate(
            flops=12 * width * half * count,
            bytes_accessed=2 * width * (2 * count + 6 * half),
            transcendentals=2 * count * half,
        ),
        name="experts",
    )(rows, *weights, *downs)


def layer(
    mix_tokens,
    mix_gain,
    value_weight,
    inner_weight,
    outer_weight,
    conv_taps,
    mix_weight,
    moe_tokens,
    moe_gain,
    router_group,
    router_expert,
    expert_routes,
    gate_weight,
    up_weight,
    down_weight,
):
    z_index = lax.axis_index("z")
    core = lax.axis_index("core")
    zs = lax.axis_size("z")
    eps = lax.axis_size(EP)
    width = moe_tokens.shape[1]
    core_ref = core.reshape(1).astype(jnp.int32)

    before = lax.ppermute(
        mix_tokens[mix_tokens.shape[0] - MOE_SHARE :], EP, [(i, i + 1) for i in range(eps - 1)]
    )
    gate, up, down = gate_weight[0], up_weight[0], down_weight[0]

    placed, half_normed, half_ranks = prepare(
        core_ref, moe_tokens, moe_gain, expert_routes, zs
    )
    placed, before = lax.optimization_barrier((placed, before))

    def exchange(array):
        return lax.all_to_all(array, EP, split_axis=0, concat_axis=0, tiled=True)

    arrived = exchange(placed.reshape(EXPERTS, CAP * zs, width)).reshape(-1, width)

    taps = (conv_taps, swap_cores(conv_taps))
    projections = (
        value_weight,
        swap_cores(value_weight),
        inner_weight,
        swap_cores(inner_weight),
        outer_weight,
        swap_cores(outer_weight),
    )
    mixes = (mix_weight, swap_cores(mix_weight))
    partial_mix = mixer_partial(
        core_ref, mix_tokens, before, mix_gain, taps, projections, mixes, zs
    )
    mixer_out = lax.psum_scatter(partial_mix, "z", scatter_dimension=0, tiled=True)

    weights = (gate, swap_cores(gate), up, swap_cores(up))
    downs = (down, swap_cores(down))
    partial_value = expert_partial(arrived, weights, downs, zs)
    partial_value, mixer_out = lax.optimization_barrier((partial_value, mixer_out))
    summed = lax.psum_scatter(partial_value, "z", scatter_dimension=0, tiled=True)
    returned = exchange(summed.reshape(eps, CAP * width // 128, 128)).reshape(-1, width)

    own_routes = lax.dynamic_slice_in_dim(
        expert_routes, (2 * z_index + core) * MOE_SHARE, MOE_SHARE, 0
    )
    own_normed = lax.dynamic_slice_in_dim(half_normed, z_index * MOE_SHARE, MOE_SHARE, 0)
    own_ranks = lax.dynamic_slice_in_dim(half_ranks, z_index * MOE_SHARE, MOE_SHARE, 1).T
    token_weights = route_weights(own_normed, own_routes, router_group, router_expert)

    position = own_routes * CAP + own_ranks
    targets = jnp.arange(EXPERTS * CAP, dtype=jnp.int32)
    spread = jnp.sum(
        jnp.where(position[:, :, None] == targets, token_weights[:, :, None], 0.0), axis=1
    )
    expert_out = jnp.dot(
        spread,
        returned.astype(jnp.float32),
        precision=lax.Precision.HIGHEST,
        preferred_element_type=jnp.float32,
    )
    return (mixer_out, expert_out.astype(jnp.bfloat16))


def solution(mesh):
    torus = Mesh(mesh.devices.reshape(4, 4, 8, 2), ALL)
    return jax.shard_map(
        layer,
        mesh=torus,
        in_specs=(
            P(EP, None),
            P(),
            P(None, TP),
            P(None, TP),
            P(None, TP),
            P(None, TP),
            P(TP, None),
            P(EP, None),
            P(),
            P(),
            P(),
            P(EP, None),
            P(EP, None, TP),
            P(EP, None, TP),
            P(EP, TP, None),
        ),
        out_specs=(P(ALL, None), P(ALL, None)),
        check_vma=False,
    )
```

```python
import functools

import jax
import jax.numpy as jnp
from jax import lax
from jax.experimental import pallas as pl
from jax.experimental.pallas import tpu as pltpu
from jax.sharding import Mesh
from jax.sharding import PartitionSpec as P


TAPS = 3
EXPERTS = 16
GROUPS = 4
TOPK = 2
MOE_SHARE = 16
EPG = 4
CAP = 4


EP = ("y", "x")
TP = ("z", "core")
ALL = EP + TP


def route_weights(normed, routes, router_group, router_expert):
    group_logit = jnp.dot(normed, router_group, preferred_element_type=jnp.float32)
    expert_logit = jnp.dot(normed, router_expert, preferred_element_type=jnp.float32)
    group_exp = jnp.exp(group_logit)
    group_id = routes[:, 0] // EPG
    group_pick = (group_id[:, None] == jnp.arange(GROUPS, dtype=jnp.int32)[None, :]).astype(
        jnp.float32
    )
    group_gate = jnp.sum(group_exp * group_pick, axis=1) / jnp.sum(group_exp, axis=1)
    expert_pick = (
        routes[:, :, None] == jnp.arange(EXPERTS, dtype=jnp.int32)[None, None, :]
    ).astype(jnp.float32)
    chosen = jnp.exp(jnp.sum(expert_logit[:, None, :] * expert_pick, axis=2))
    return group_gate[:, None] * chosen / jnp.sum(chosen, axis=1, keepdims=True)


def swap_cores(value):
    return lax.ppermute(value, "core", [(0, 1), (1, 0)])


def iota(shape, dim):
    return lax.broadcasted_iota(jnp.int32, shape, dim)


def select_matrix(mask):
    return jnp.where(mask, 1.0, 0.0).astype(jnp.bfloat16)


def product(left, right):
    return jnp.dot(left, right, preferred_element_type=jnp.float32)


def scaled_rows(rows, gain):
    values = rows.astype(jnp.float32)
    inverse = lax.rsqrt(jnp.mean(values * values, axis=-1, keepdims=True) + 1e-06)
    return (values * inverse * gain).astype(jnp.bfloat16)


def prep_kernel(zs, place_ref, tokens_ref, gain_ref, routes_ref, placed_ref, normed_ref, ranks_ref):
    share = MOE_SHARE
    rows = zs * share
    width = tokens_ref.shape[-1]
    normed_ref[...] = scaled_rows(tokens_ref[...].reshape(rows, width), gain_ref[...])
    token = iota((2 * rows, rows), 1)
    source = (token // share) * (2 * share) + place_ref[0] * share + token % share
    pick = select_matrix(iota((2 * rows, rows), 0) == source)
    routes = product(routes_ref[...].astype(jnp.float32).astype(jnp.bfloat16), pick).astype(jnp.int32)
    expert = iota((EXPERTS, rows), 0)
    named = [expert == routes[k : k + 1] for k in range(TOPK)]
    earlier, later = iota((rows, rows), 0), iota((rows, rows), 1)
    before = (earlier // share == later // share) & (earlier < later)
    counts = product(select_matrix(named[0] | named[1]), select_matrix(before))
    ranks = [
        jnp.sum(jnp.where(named[k], counts, 0.0), axis=0, keepdims=True).astype(jnp.int32)
        for k in range(TOPK)
    ]
    block = iota((1, rows), 1) // share
    part = CAP // 2
    slots = iota((EXPERTS * part * zs, rows), 0)
    inside = []
    for k in range(TOPK):
        ranks_ref[k : k + 1, :] = ranks[k]
        slot = ranks[k] - part * (place_ref[1] % 2)
        held = (slot >= 0) & (slot < part)
        spot = (routes[k : k + 1] * part + slot) * zs + block
        inside.append(slots == jnp.where(held, spot, -1))
    select = select_matrix(inside[0] | inside[1])
    step = 512

    @pl.loop(0, width // step)
    def _(index):
        columns = pl.ds(pl.multiple_of(index * step, step), step)
        placed_ref[:, columns] = product(select, normed_ref[:, columns]).astype(jnp.bfloat16)


def prepare(place, tokens, gain, routes, zs):
    rows, width = tokens.shape
    half = rows // 2
    return pl.pallas_call(
        functools.partial(prep_kernel, zs),
        grid_spec=pltpu.PrefetchScalarGridSpec(
            num_scalar_prefetch=1,
            grid=(1,),
            in_specs=[
                pl.BlockSpec((zs, 1, MOE_SHARE, width), lambda i, c: (0, c[0], 0, 0)),
                pl.BlockSpec((1, width), lambda i, c: (0, 0)),
                pl.BlockSpec((TOPK, rows), lambda i, c: (0, 0)),
            ],
            out_specs=[
                pl.BlockSpec((EXPERTS * (CAP // 2) * zs, width), lambda i, c: (0, 0)),
                pl.BlockSpec((half, width), lambda i, c: (0, 0)),
                pl.BlockSpec((TOPK, half), lambda i, c: (0, 0)),
            ],
        ),
        out_shape=[
            jax.ShapeDtypeStruct((EXPERTS * (CAP // 2) * zs, width), jnp.bfloat16),
            jax.ShapeDtypeStruct((half, width), jnp.bfloat16),
            jax.ShapeDtypeStruct((TOPK, half), jnp.int32),
        ],
        cost_estimate=pl.CostEstimate(
            flops=2 * EXPERTS * (CAP // 2) * zs * half * width,
            bytes_accessed=2 * width * (rows + EXPERTS * (CAP // 2) * zs),
            transcendentals=0,
        ),
        name="prepare",
    )(
        place,
        tokens.reshape(zs, 2, MOE_SHARE, width),
        gain.reshape(1, width),
        routes.T,
    )


def mixer_kernel(
    steps, core_ref, tokens_ref, halo_ref, before_ref, gain_ref, taps_mine, taps_theirs, *refs
):
    weights, (m0, m1, out_ref, normed_ref, sums_ref, channels_ref) = refs[:6], refs[6:]
    step = pl.program_id(0)
    rows = out_ref.shape[0]
    depth, half = weights[0].shape
    width = tokens_ref.shape[-1]
    blocks, _, tail_rows, _ = halo_ref.shape
    halos = blocks * tail_rows
    total = normed_ref.shape[0]
    reach = TAPS - 1

    @pl.when(step == 0)
    def _():
        gain = gain_ref[...]
        normed_ref[0:rows, :] = scaled_rows(tokens_ref[...].reshape(rows, width), gain)
        normed_ref[rows : rows + halos, :] = scaled_rows(halo_ref[...].reshape(halos, width), gain)
        normed_ref[rows + halos :, :] = scaled_rows(before_ref[...], gain)
        sums_ref[...] = jnp.zeros_like(sums_ref)

    @pl.when(step < steps)
    def _():
        piece = normed_ref[:, pl.ds(pl.multiple_of(step * depth, depth), depth)]
        joint = jnp.concatenate([weight[...] for weight in weights], axis=1)
        sums_ref[...] += product(piece, joint)

    @pl.when(step == steps - 1)
    def _():
        def pair(index):
            return sums_ref[:, 2 * index * half : 2 * (index + 1) * half]

        gated = (pair(1) * pair(0)).astype(jnp.bfloat16)
        row, source = iota((rows, total), 0), iota((rows, total), 1)
        place = row % MOE_SHARE
        ahead = row // MOE_SHARE + core_ref[0]
        tail = jnp.where(ahead == 0, total, rows + ahead * tail_rows)
        taps = jnp.concatenate([taps_mine[...], taps_theirs[...]], axis=1)
        mixed = None
        for tap in range(TAPS):
            back = reach - tap
            wanted = jnp.where(place >= back, row, tail + place) - back
            shifted = product(select_matrix(source == wanted), gated)
            term = taps[tap : tap + 1] * shifted
            mixed = term if mixed is None else mixed + term
        channels_ref[...] = (pair(2)[0:rows] * mixed).astype(jnp.bfloat16)

    @pl.when(step >= steps)
    def _():
        joint = jnp.concatenate([m0[...], m1[...]], axis=0)
        out_ref[...] = product(channels_ref[...], joint).astype(jnp.bfloat16)


def mixer_partial(core, tokens, before, gain, taps, weights, mixes, zs):
    rows, width = tokens.shape
    half = rows // 2
    channels = weights[0].shape[1]
    depth = 1024
    steps = width // depth
    tail_rows = MOE_SHARE // 2
    total = half + zs * tail_rows + before.shape[0]
    fixed = lambda i, c: (0, 0)
    after = lambda i, c: (0, jnp.maximum(i - steps, 0))
    split = tokens.reshape(zs, 2, MOE_SHARE, width)
    return pl.pallas_call(
        functools.partial(mixer_kernel, steps),
        grid_spec=pltpu.PrefetchScalarGridSpec(
            num_scalar_prefetch=1,
            grid=(2 * steps,),
            in_specs=[
                pl.BlockSpec((zs, 1, MOE_SHARE, width), lambda i, c: (0, c[0], 0, 0)),
                pl.BlockSpec((zs, 1, tail_rows, width), lambda i, c: (0, 1 - c[0], 1, 0)),
                pl.BlockSpec(before.shape, fixed),
                pl.BlockSpec((1, width), fixed),
                pl.BlockSpec((TAPS, channels), fixed),
                pl.BlockSpec((TAPS, channels), fixed),
            ]
            + [pl.BlockSpec((depth, channels), lambda i, c: (jnp.minimum(i, steps - 1), 0))] * 6
            + [pl.BlockSpec((channels, depth), after)] * 2,
            out_specs=pl.BlockSpec((half, depth), after),
            scratch_shapes=[
                pltpu.VMEM((total, width), jnp.bfloat16),
                pltpu.VMEM((total, 6 * channels), jnp.float32),
                pltpu.VMEM((half, 2 * channels), jnp.bfloat16),
            ],
        ),
        out_shape=jax.ShapeDtypeStruct((half, width), jnp.bfloat16),
        cost_estimate=pl.CostEstimate(
            flops=2 * width * channels * (6 * total + 2 * half),
            bytes_accessed=2 * width * (total + half + 8 * channels),
            transcendentals=0,
        ),
        name="mixer",
    )(core, split, split, before, gain.reshape(1, width), *taps, *weights, *mixes)


def gated_units(sums):
    units = sums.shape[1] // 2
    gate, up = sums[:, :units], sums[:, units:]
    return (gate * jax.nn.sigmoid(gate) * up).astype(jnp.bfloat16)


def units_kernel(steps, rows_ref, g0, g1, u0, u1, out_ref, sums_ref):
    step = pl.program_id(0)
    joint = jnp.concatenate([g0[...], g1[...], u0[...], u1[...]], axis=1)
    piece = product(rows_ref[...], joint)

    @pl.when(step == 0)
    def _():
        sums_ref[...] = piece

    @pl.when(step > 0)
    def _():
        sums_ref[...] += piece

    @pl.when(step == steps - 1)
    def _():
        out_ref[...] = gated_units(sums_ref[...])


def expert_units(rows, weights):
    count, width = rows.shape
    half = weights[0].shape[1]
    depth = 1024
    steps = width // depth
    return pl.pallas_call(
        functools.partial(units_kernel, steps),
        grid=(steps,),
        in_specs=[pl.BlockSpec((count, depth), lambda i: (0, i))]
        + [pl.BlockSpec((depth, half), lambda i: (i, 0))] * 4,
        out_specs=pl.BlockSpec((count, 2 * half), lambda i: (0, 0)),
        scratch_shapes=[pltpu.VMEM((count, 4 * half), jnp.float32)],
        out_shape=jax.ShapeDtypeStruct((count, 2 * half), jnp.bfloat16),
        cost_estimate=pl.CostEstimate(
            flops=8 * width * half * count,
            bytes_accessed=2 * width * (count + 4 * half),
            transcendentals=2 * count * half,
        ),
        name="units",
    )(rows, *weights)


def expert_kernel(
    zs, steps, place_ref, before_ref, after_ref, own_ref, g0, g1, u0, u1, d0, d1, out_ref,
    sums_ref, units_ref
):
    step = pl.program_id(0)
    count = own_ref.shape[0]
    given = units_ref.shape[0]

    @pl.when(step < steps)
    def _():
        joint = jnp.concatenate([g0[...], g1[...], u0[...], u1[...]], axis=1)
        rows = jnp.concatenate([before_ref[...], after_ref[...]], axis=0)
        piece = product(rows, joint)

        @pl.when(step == 0)
        def _():
            sums_ref[...] = piece

        @pl.when(step > 0)
        def _():
            sums_ref[...] += piece

    @pl.when(step == steps - 1)
    def _():
        part = CAP // 2
        target, source = iota((given, count), 0), iota((given, count), 1)
        line = source // zs
        first = (source % zs) * (given // zs) + (line // part) * CAP + line % part
        odd = place_ref[1] % 2
        own = select_matrix(target == first + part * odd)
        other = select_matrix(target == first + part * (1 - odd))
        units_ref[...] = (
            product(own, own_ref[...]) + product(other, gated_units(sums_ref[...]))
        ).astype(jnp.bfloat16)

    @pl.when(step >= steps)
    def _():
        joint = jnp.concatenate([d0[...], d1[...]], axis=0)
        out_ref[...] = product(units_ref[...], joint).astype(jnp.bfloat16)


def expert_partial(place, before, after, own_units, weights, downs, zs):
    rows, width = before.shape
    count = own_units.shape[0]
    given = 2 * count
    half = weights[0].shape[1]
    depth = 1024
    steps = width // depth
    early = lambda i: jnp.minimum(i, steps - 1)
    late = lambda i: jnp.maximum(i - steps, 0)
    return pl.pallas_call(
        functools.partial(expert_kernel, zs, steps),
        grid_spec=pltpu.PrefetchScalarGridSpec(
            num_scalar_prefetch=1,
            grid=(2 * steps,),
            in_specs=[pl.BlockSpec((rows, depth), lambda i, p: (0, early(i)))] * 2
            + [pl.BlockSpec((count, 2 * half), lambda i, p: (0, 0))]
            + [pl.BlockSpec((depth, half), lambda i, p: (early(i), 0))] * 4
            + [pl.BlockSpec((half, depth), lambda i, p: (0, late(i)))] * 2,
            out_specs=pl.BlockSpec((given, depth), lambda i, p: (0, late(i))),
            scratch_shapes=[
                pltpu.VMEM((count, 4 * half), jnp.float32),
                pltpu.VMEM((given, 2 * half), jnp.bfloat16),
            ],
        ),
        out_shape=jax.ShapeDtypeStruct((given, width), jnp.bfloat16),
        cost_estimate=pl.CostEstimate(
            flops=8 * width * half * count + 4 * width * half * given,
            bytes_accessed=2 * width * (count + given + 6 * half),
            transcendentals=2 * count * half,
        ),
        name="experts",
    )(place, before, after, own_units, *weights, *downs)


def layer(
    mix_tokens,
    mix_gain,
    value_weight,
    inner_weight,
    outer_weight,
    conv_taps,
    mix_weight,
    moe_tokens,
    moe_gain,
    router_group,
    router_expert,
    expert_routes,
    gate_weight,
    up_weight,
    down_weight,
):
    z_index = lax.axis_index("z")
    core = lax.axis_index("core")
    zs = lax.axis_size("z")
    eps = lax.axis_size(EP)
    width = moe_tokens.shape[1]
    core_ref = jnp.stack([core, z_index]).astype(jnp.int32)

    before = lax.ppermute(
        mix_tokens[mix_tokens.shape[0] - MOE_SHARE :], EP, [(i, i + 1) for i in range(eps - 1)]
    )
    gate, up, down = gate_weight[0], up_weight[0], down_weight[0]

    placed, half_normed, half_ranks = prepare(
        core_ref, moe_tokens, moe_gain, expert_routes, zs
    )
    placed, before = lax.optimization_barrier((placed, before))

    def exchange(array):
        return lax.all_to_all(array, EP, split_axis=0, concat_axis=0, tiled=True)

    arrived = exchange(placed.reshape(EXPERTS, CAP // 2 * zs, width)).reshape(-1, width)

    taps = (conv_taps, swap_cores(conv_taps))
    projections = (
        value_weight,
        swap_cores(value_weight),
        inner_weight,
        swap_cores(inner_weight),
        outer_weight,
        swap_cores(outer_weight),
    )
    mixes = (mix_weight, swap_cores(mix_weight))
    partial_mix = mixer_partial(
        core_ref, mix_tokens, before, mix_gain, taps, projections, mixes, zs
    )
    mixer_out = lax.psum_scatter(partial_mix, "z", scatter_dimension=0, tiled=True)

    weights = (gate, swap_cores(gate), up, swap_cores(up))
    downs = (down, swap_cores(down))
    middle = arrived.shape[0] // 2
    from_before = lax.ppermute(arrived[:middle], "z", [(i, (i + 1) % zs) for i in range(zs)])
    from_after = lax.ppermute(arrived[middle:], "z", [(i, (i - 1) % zs) for i in range(zs)])
    own_units = expert_units(arrived, weights)
    partial_value = expert_partial(
        core_ref, from_before, from_after, own_units, weights, downs, zs
    )
    partial_value, mixer_out = lax.optimization_barrier((partial_value, mixer_out))
    summed = lax.psum_scatter(partial_value, "z", scatter_dimension=0, tiled=True)
    returned = exchange(summed.reshape(eps, CAP * width // 128, 128)).reshape(-1, width)

    own_routes = lax.dynamic_slice_in_dim(
        expert_routes, (2 * z_index + core) * MOE_SHARE, MOE_SHARE, 0
    )
    own_normed = lax.dynamic_slice_in_dim(half_normed, z_index * MOE_SHARE, MOE_SHARE, 0)
    own_ranks = lax.dynamic_slice_in_dim(half_ranks, z_index * MOE_SHARE, MOE_SHARE, 1).T
    token_weights = route_weights(own_normed, own_routes, router_group, router_expert)

    position = own_routes * CAP + own_ranks
    targets = jnp.arange(EXPERTS * CAP, dtype=jnp.int32)
    spread = jnp.sum(
        jnp.where(position[:, :, None] == targets, token_weights[:, :, None], 0.0), axis=1
    )
    expert_out = jnp.dot(
        spread,
        returned.astype(jnp.float32),
        precision=lax.Precision.HIGHEST,
        preferred_element_type=jnp.float32,
    )
    return (mixer_out, expert_out.astype(jnp.bfloat16))


def solution(mesh):
    torus = Mesh(mesh.devices.reshape(4, 4, 8, 2), ALL)
    return jax.shard_map(
        layer,
        mesh=torus,
        in_specs=(
            P(EP, None),
            P(),
            P(None, TP),
            P(None, TP),
            P(None, TP),
            P(None, TP),
            P(TP, None),
            P(EP, None),
            P(),
            P(),
            P(),
            P(EP, None),
            P(EP, None, TP),
            P(EP, None, TP),
            P(EP, TP, None),
        ),
        out_specs=(P(ALL, None), P(ALL, None)),
        check_vma=False,
    )
```

```python
import functools

import jax
import jax.numpy as jnp
from jax import lax
from jax.experimental import pallas as pl
from jax.experimental.pallas import tpu as pltpu
from jax.sharding import Mesh
from jax.sharding import PartitionSpec as P


TAPS = 3
EXPERTS = 16
GROUPS = 4
TOPK = 2
MOE_SHARE = 16
EPG = 4
CAP = 4


MIX_CHAINS = 2

EP = ("y", "x")
TP = ("z", "core")
ALL = EP + TP


def route_weights(normed, routes, router_group, router_expert):
    group_logit = jnp.dot(normed, router_group, preferred_element_type=jnp.float32)
    expert_logit = jnp.dot(normed, router_expert, preferred_element_type=jnp.float32)
    group_exp = jnp.exp(group_logit)
    group_id = routes[:, 0] // EPG
    group_pick = (group_id[:, None] == jnp.arange(GROUPS, dtype=jnp.int32)[None, :]).astype(
        jnp.float32
    )
    group_gate = jnp.sum(group_exp * group_pick, axis=1) / jnp.sum(group_exp, axis=1)
    expert_pick = (
        routes[:, :, None] == jnp.arange(EXPERTS, dtype=jnp.int32)[None, None, :]
    ).astype(jnp.float32)
    chosen = jnp.exp(jnp.sum(expert_logit[:, None, :] * expert_pick, axis=2))
    return group_gate[:, None] * chosen / jnp.sum(chosen, axis=1, keepdims=True)


def swap_cores(value):
    return lax.ppermute(value, "core", [(0, 1), (1, 0)])


def swap_late(value):
    return lax.ppermute(value, "core", [(0, 1), (1, 0)])


def iota(shape, dim):
    return lax.broadcasted_iota(jnp.int32, shape, dim)


def select_matrix(mask):
    return jnp.where(mask, 1.0, 0.0).astype(jnp.bfloat16)


def product(left, right):
    return jnp.dot(left, right, preferred_element_type=jnp.float32)


def scaled_rows(rows, gain):
    values = rows.astype(jnp.float32)
    inverse = lax.rsqrt(jnp.mean(values * values, axis=-1, keepdims=True) + 1e-06)
    return (values * inverse * gain).astype(jnp.bfloat16)


def prep_kernel(
    zs, place_ref, tokens_ref, gain_ref, routes_ref, placed_ref, own_ref, ranks_ref,
    normed_ref, select_ref
):
    share = MOE_SHARE
    rows = zs * share
    width = tokens_ref.shape[-1]
    step = pl.program_id(0)

    @pl.when(step == 0)
    def _():
        normed_ref[...] = scaled_rows(tokens_ref[...].reshape(rows, width), gain_ref[...])
        own_ref[...] = normed_ref[pl.ds(pl.multiple_of(place_ref[1] * share, share), share), :]
        token = iota((1, rows), 1)
        block = token // share
        source = block * (2 * share) + place_ref[0] * share + token % share
        pick = select_matrix(iota((2 * rows, 1), 0) == source)
        routes = routes_ref[...].astype(jnp.float32).astype(jnp.bfloat16)
        routes = product(routes, pick).astype(jnp.int32)
        expert = iota((EXPERTS, 1), 0)
        named = [expert == routes[k : k + 1] for k in range(TOPK)]
        earlier = iota((rows, 1), 0)
        before = (earlier // share == block) & (earlier < token)
        counts = product(select_matrix(named[0] | named[1]), select_matrix(before))
        slots = iota((EXPERTS * CAP * zs, 1), 0)
        inside = []
        for k in range(TOPK):
            ranks = jnp.sum(jnp.where(named[k], counts, 0.0), axis=0, keepdims=True)
            ranks = ranks.astype(jnp.int32)
            ranks_ref[k : k + 1, :] = ranks
            inside.append(slots == (routes[k : k + 1] * CAP + ranks) * zs + block)
        select_ref[...] = select_matrix(inside[0] | inside[1])

    depth = placed_ref.shape[1]
    columns = pl.ds(pl.multiple_of(step * depth, depth), depth)
    placed_ref[...] = product(select_ref[...], normed_ref[:, columns]).astype(jnp.bfloat16)


def prepare(place, tokens, gain, routes, zs):
    rows, width = tokens.shape
    half = rows // 2
    depth = 1024
    placed = EXPERTS * CAP * zs
    fixed = lambda i, p: (0, 0)
    return pl.pallas_call(
        functools.partial(prep_kernel, zs),
        grid_spec=pltpu.PrefetchScalarGridSpec(
            num_scalar_prefetch=1,
            grid=(width // depth,),
            in_specs=[
                pl.BlockSpec((zs, 1, MOE_SHARE, width), lambda i, p: (0, p[0], 0, 0)),
                pl.BlockSpec((1, width), fixed),
                pl.BlockSpec((TOPK, rows), fixed),
            ],
            out_specs=[
                pl.BlockSpec((placed, depth), lambda i, p: (0, i)),
                pl.BlockSpec((MOE_SHARE, width), fixed),
                pl.BlockSpec((TOPK, half), fixed),
            ],
            scratch_shapes=[
                pltpu.VMEM((half, width), jnp.bfloat16),
                pltpu.VMEM((placed, half), jnp.bfloat16),
            ],
        ),
        out_shape=[
            jax.ShapeDtypeStruct((placed, width), jnp.bfloat16),
            jax.ShapeDtypeStruct((MOE_SHARE, width), jnp.bfloat16),
            jax.ShapeDtypeStruct((TOPK, half), jnp.int32),
        ],
        cost_estimate=pl.CostEstimate(
            flops=2 * placed * half * width,
            bytes_accessed=2 * width * (half + placed),
            transcendentals=0,
        ),
        name="prepare",
    )(
        place,
        tokens.reshape(zs, 2, MOE_SHARE, width),
        gain.reshape(1, width),
        routes.T,
    )


def mixer_kernel(
    steps, place_ref, tokens_ref, halo_ref, before_ref, gain_ref, taps_mine, taps_theirs, *refs
):
    weights, (m0, m1), outs = refs[:6], refs[6:8], refs[8:-3]
    normed_ref, sums_ref, channels_ref = refs[-3:]
    step = pl.program_id(0)
    rows = channels_ref.shape[0]
    depth, half = weights[0].shape
    width = tokens_ref.shape[-1]
    blocks, _, tail_rows, _ = halo_ref.shape
    halos = blocks * tail_rows
    total = normed_ref.shape[0]
    reach = TAPS - 1

    @pl.when(step == 0)
    def _():
        gain = gain_ref[...]
        normed_ref[0:rows, :] = scaled_rows(tokens_ref[...].reshape(rows, width), gain)
        normed_ref[rows : rows + halos, :] = scaled_rows(halo_ref[...].reshape(halos, width), gain)
        normed_ref[rows + halos :, :] = scaled_rows(before_ref[...], gain)
        sums_ref[...] = jnp.zeros_like(sums_ref)

    @pl.when(step < steps)
    def _():
        piece = normed_ref[:, pl.ds(pl.multiple_of(step * depth, depth), depth)]
        joint = jnp.concatenate([weight[...] for weight in weights], axis=1)
        sums_ref[...] += product(piece, joint)

    @pl.when(step == steps - 1)
    def _():
        def pair(index):
            return sums_ref[:, 2 * index * half : 2 * (index + 1) * half]

        gated = (pair(1) * pair(0)).astype(jnp.bfloat16)
        row, source = iota((rows, 1), 0), iota((1, total), 1)
        place = row % MOE_SHARE
        ahead = row // MOE_SHARE + place_ref[0]
        tail = jnp.where(ahead == 0, total, rows + ahead * tail_rows)
        taps = jnp.concatenate([taps_mine[...], taps_theirs[...]], axis=1)
        mixed = None
        for tap in range(TAPS):
            back = reach - tap
            wanted = jnp.where(place >= back, row, tail + place) - back
            shifted = product(select_matrix(source == wanted), gated)
            term = taps[tap : tap + 1] * shifted
            mixed = term if mixed is None else mixed + term
        channels = (pair(2)[0:rows] * mixed).astype(jnp.bfloat16)
        target, source = iota((rows, 1), 0), iota((1, rows), 1)
        turned = (source // MOE_SHARE - place_ref[1] + blocks) % blocks
        order = select_matrix(target == turned * MOE_SHARE + source % MOE_SHARE)
        channels_ref[...] = product(order, channels).astype(jnp.bfloat16)

    write_chains(step - steps, MOE_SHARE, outs, lambda: product(
        channels_ref[...], jnp.concatenate([m0[...], m1[...]], axis=0)
    ))


def write_chains(step, rows, outs, compute):
    chains = len(outs) // 2
    pieces = chains * outs[0].shape[1] // 1024
    for piece in range(pieces):
        chain = piece * chains // pieces
        whole, sent = outs[chain], outs[chains + chain]
        start = (piece * 1024) % whole.shape[1]
        first = whole.shape[0] - rows if chain % 2 == 0 else rows

        @pl.when(step == piece)
        def _():
            total = compute().astype(jnp.bfloat16)
            whole[:, start : start + 1024] = total
            sent[:, start : start + 1024] = total[first : first + rows]


def chain_outputs(count, rows, width, chains):
    shapes = [(count, width // chains)] * chains + [(rows, width // chains)] * chains
    return (
        [pl.BlockSpec(shape, lambda *_: (0, 0)) for shape in shapes],
        [jax.ShapeDtypeStruct(shape, jnp.bfloat16) for shape in shapes],
    )


def ring_sum(outs):
    chains = len(outs) // 2
    wholes, sums = outs[:chains], list(outs[chains:])
    rows = sums[0].shape[0]
    zs = lax.axis_size("z")
    for hop in range(zs - 1):
        for chain in range(chains):
            way = 1 if chain % 2 == 0 else -1
            came = lax.ppermute(sums[chain], "z", [(i, (i + way) % zs) for i in range(zs)])
            block = (zs - 2 - hop) if way == 1 else (hop + 2) % zs
            mine = wholes[chain][block * rows : (block + 1) * rows]
            total = came.astype(jnp.float32) + mine.astype(jnp.float32)
            sums[chain] = total.astype(jnp.bfloat16)
    return sums


def mixer_partial(place, tokens, before, gain, taps, weights, mixes, zs):
    rows, width = tokens.shape
    half = rows // 2
    channels = weights[0].shape[1]
    depth = 1024
    steps = width // depth
    tail_rows = MOE_SHARE // 2
    total = half + zs * tail_rows + before.shape[0]
    fixed = lambda i, c: (0, 0)
    after = lambda i, c: (0, jnp.maximum(i - steps, 0))
    out_specs, out_shape = chain_outputs(half, MOE_SHARE, width, MIX_CHAINS)
    split = tokens.reshape(zs, 2, MOE_SHARE, width)
    return pl.pallas_call(
        functools.partial(mixer_kernel, steps),
        grid_spec=pltpu.PrefetchScalarGridSpec(
            num_scalar_prefetch=1,
            grid=(2 * steps,),
            in_specs=[
                pl.BlockSpec((zs, 1, MOE_SHARE, width), lambda i, c: (0, c[0], 0, 0)),
                pl.BlockSpec((zs, 1, tail_rows, width), lambda i, c: (0, 1 - c[0], 1, 0)),
                pl.BlockSpec(before.shape, fixed),
                pl.BlockSpec((1, width), fixed),
                pl.BlockSpec((TAPS, channels), fixed),
                pl.BlockSpec((TAPS, channels), fixed),
            ]
            + [pl.BlockSpec((depth, channels), lambda i, c: (jnp.minimum(i, steps - 1), 0))] * 6
            + [pl.BlockSpec((channels, depth), after)] * 2,
            out_specs=out_specs,
            scratch_shapes=[
                pltpu.VMEM((total, width), jnp.bfloat16),
                pltpu.VMEM((total, 6 * channels), jnp.float32),
                pltpu.VMEM((half, 2 * channels), jnp.bfloat16),
            ],
        ),
        out_shape=out_shape,
        cost_estimate=pl.CostEstimate(
            flops=2 * width * channels * (6 * total + 2 * half),
            bytes_accessed=2 * width * (total + half + 8 * channels),
            transcendentals=0,
        ),
        name="mixer",
    )(place, split, split, before, gain.reshape(1, width), *taps, *weights, *mixes)


def expert_kernel(zs, steps, rows_ref, g0, g1, u0, u1, d0, d1, out_ref, sums_ref, units_ref):
    step = pl.program_id(0)
    count = rows_ref.shape[0]
    units = 2 * g0.shape[1]

    @pl.when(step == 0)
    def _():
        sums_ref[...] = jnp.zeros_like(sums_ref)

    @pl.when(step < steps)
    def _():
        joint = jnp.concatenate([g0[...], g1[...], u0[...], u1[...]], axis=1)
        sums_ref[...] += product(rows_ref[...], joint)

    @pl.when(step == steps - 1)
    def _():
        target, source = iota((count, 1), 0), iota((1, count), 1)
        order = select_matrix(target == (source % zs) * (count // zs) + source // zs)
        gate, up = sums_ref[:, :units], sums_ref[:, units:]
        hidden = (gate * jax.nn.sigmoid(gate) * up).astype(jnp.bfloat16)
        units_ref[...] = product(order, hidden).astype(jnp.bfloat16)

    @pl.when(step >= steps)
    def _():
        joint = jnp.concatenate([d0[...], d1[...]], axis=0)
        out_ref[...] = product(units_ref[...], joint).astype(jnp.bfloat16)


def expert_partial(rows, weights, downs, zs):
    count, width = rows.shape
    half = weights[0].shape[1]
    depth = 1024
    steps = width // depth
    early = lambda i: jnp.minimum(i, steps - 1)
    after = lambda i: jnp.maximum(i - steps, 0)
    return pl.pallas_call(
        functools.partial(expert_kernel, zs, steps),
        grid=(2 * steps,),
        in_specs=[pl.BlockSpec((count, depth), lambda i: (0, early(i)))]
        + [pl.BlockSpec((depth, half), lambda i: (early(i), 0))] * 4
        + [pl.BlockSpec((half, depth), lambda i: (0, after(i)))] * 2,
        out_specs=pl.BlockSpec((count, depth), lambda i: (0, after(i))),
        scratch_shapes=[
            pltpu.VMEM((count, 4 * half), jnp.float32),
            pltpu.VMEM((count, 2 * half), jnp.bfloat16),
        ],
        out_shape=jax.ShapeDtypeStruct((count, width), jnp.bfloat16),
        cost_estimate=pl.CostEstimate(
            flops=12 * width * half * count,
            bytes_accessed=2 * width * (2 * count + 6 * half),
            transcendentals=2 * count * half,
        ),
        name="experts",
    )(rows, *weights, *downs)


def layer(
    mix_tokens,
    mix_gain,
    value_weight,
    inner_weight,
    outer_weight,
    conv_taps,
    mix_weight,
    moe_tokens,
    moe_gain,
    router_group,
    router_expert,
    expert_routes,
    gate_weight,
    up_weight,
    down_weight,
):
    z_index = lax.axis_index("z")
    core = lax.axis_index("core")
    zs = lax.axis_size("z")
    eps = lax.axis_size(EP)
    width = moe_tokens.shape[1]
    core_ref = jnp.stack([core, z_index]).astype(jnp.int32)

    gate, up, down = gate_weight[0], up_weight[0], down_weight[0]
    theirs = [swap_cores(array) for array in (gate, up, down)]

    placed, own_normed, half_ranks = prepare(
        core_ref, moe_tokens, moe_gain, expert_routes, zs
    )
    placed, own_normed, half_ranks, theirs = lax.optimization_barrier(
        (placed, own_normed, half_ranks, theirs)
    )

    def exchange(array):
        return lax.all_to_all(array, EP, split_axis=0, concat_axis=0, tiled=True)

    arrived = exchange(placed.reshape(EXPERTS, CAP * zs, width)).reshape(-1, width)
    partial_value = expert_partial(arrived, (gate, theirs[0], up, theirs[1]), (down, theirs[2]), zs)
    summed = lax.psum_scatter(partial_value, "z", scatter_dimension=0, tiled=True)

    _, later = lax.optimization_barrier(
        (
            partial_value,
            (
                mix_tokens,
                (value_weight, inner_weight, outer_weight),
                (conv_taps, mix_weight),
                own_normed,
                half_ranks,
                expert_routes,
            ),
        )
    )
    mix_tokens, projections, (conv_taps, mix_weight), own_normed, half_ranks, expert_routes = later
    before = lax.ppermute(
        mix_tokens[mix_tokens.shape[0] - MOE_SHARE :], EP, [(i, i + 1) for i in range(eps - 1)]
    )
    taps = (conv_taps, swap_late(conv_taps))
    weights = [part for array in projections for part in (array, swap_late(array))]
    mixes = (mix_weight, swap_late(mix_weight))
    partial_mix = mixer_partial(core_ref, mix_tokens, before, mix_gain, taps, weights, mixes, zs)
    mixer_out = jnp.concatenate(ring_sum(partial_mix), axis=1)
    summed, mixer_out = lax.optimization_barrier((summed, mixer_out))
    returned = exchange(summed.reshape(eps, CAP * width // 128, 128)).reshape(-1, width)

    own_routes = lax.dynamic_slice_in_dim(
        expert_routes, (2 * z_index + core) * MOE_SHARE, MOE_SHARE, 0
    )
    own_ranks = lax.dynamic_slice_in_dim(half_ranks, z_index * MOE_SHARE, MOE_SHARE, 1).T
    token_weights = route_weights(own_normed, own_routes, router_group, router_expert)

    position = own_routes * CAP + own_ranks
    targets = jnp.arange(EXPERTS * CAP, dtype=jnp.int32)
    spread = jnp.sum(
        jnp.where(position[:, :, None] == targets, token_weights[:, :, None], 0.0), axis=1
    )
    expert_out = jnp.dot(
        spread,
        returned.astype(jnp.float32),
        precision=lax.Precision.HIGHEST,
        preferred_element_type=jnp.float32,
    )
    return (mixer_out, expert_out.astype(jnp.bfloat16))


def solution(mesh):
    torus = Mesh(mesh.devices.reshape(4, 4, 8, 2), ALL)
    return jax.shard_map(
        layer,
        mesh=torus,
        in_specs=(
            P(EP, None),
            P(),
            P(None, TP),
            P(None, TP),
            P(None, TP),
            P(None, TP),
            P(TP, None),
            P(EP, None),
            P(),
            P(),
            P(),
            P(EP, None),
            P(EP, None, TP),
            P(EP, None, TP),
            P(EP, TP, None),
        ),
        out_specs=(P(ALL, None), P(ALL, None)),
        check_vma=False,
    )
```

```python
import functools

import jax
import jax.numpy as jnp
from jax import lax
from jax.experimental import pallas as pl
from jax.experimental.pallas import tpu as pltpu
from jax.sharding import Mesh
from jax.sharding import PartitionSpec as P


TAPS = 3
EXPERTS = 16
GROUPS = 4
TOPK = 2
MOE_SHARE = 16
EPG = 4
CAP = 4


MIX_CHAINS = 2

EP = ("y", "x")
TP = ("z", "core")
ALL = EP + TP


def route_weights(normed, routes, router_group, router_expert):
    group_logit = jnp.dot(normed, router_group, preferred_element_type=jnp.float32)
    expert_logit = jnp.dot(normed, router_expert, preferred_element_type=jnp.float32)
    group_exp = jnp.exp(group_logit)
    group_id = routes[:, 0] // EPG
    group_pick = (group_id[:, None] == jnp.arange(GROUPS, dtype=jnp.int32)[None, :]).astype(
        jnp.float32
    )
    group_gate = jnp.sum(group_exp * group_pick, axis=1) / jnp.sum(group_exp, axis=1)
    expert_pick = (
        routes[:, :, None] == jnp.arange(EXPERTS, dtype=jnp.int32)[None, None, :]
    ).astype(jnp.float32)
    chosen = jnp.exp(jnp.sum(expert_logit[:, None, :] * expert_pick, axis=2))
    return group_gate[:, None] * chosen / jnp.sum(chosen, axis=1, keepdims=True)


def swap_cores(value):
    return lax.ppermute(value, "core", [(0, 1), (1, 0)])


def swap_late(value):
    return lax.ppermute(value, "core", [(0, 1), (1, 0)])


def iota(shape, dim):
    return lax.broadcasted_iota(jnp.int32, shape, dim)


def select_matrix(mask):
    return jnp.where(mask, 1.0, 0.0).astype(jnp.bfloat16)


def product(left, right):
    return jnp.dot(left, right, preferred_element_type=jnp.float32)


def scaled_rows(rows, gain):
    values = rows.astype(jnp.float32)
    inverse = lax.rsqrt(jnp.mean(values * values, axis=-1, keepdims=True) + 1e-06)
    return (values * inverse * gain).astype(jnp.bfloat16)


def prep_kernel(
    zs, place_ref, tokens_ref, gain_ref, routes_ref, placed_ref, own_ref, ranks_ref,
    normed_ref, select_ref
):
    share = MOE_SHARE
    rows = zs * share
    width = tokens_ref.shape[-1]
    step = pl.program_id(0)

    @pl.when(step == 0)
    def _():
        normed_ref[...] = scaled_rows(tokens_ref[...].reshape(rows, width), gain_ref[...])
        own_ref[...] = normed_ref[pl.ds(pl.multiple_of(place_ref[1] * share, share), share), :]
        token = iota((1, rows), 1)
        block = token // share
        source = block * (2 * share) + place_ref[0] * share + token % share
        pick = select_matrix(iota((2 * rows, 1), 0) == source)
        routes = routes_ref[...].astype(jnp.float32).astype(jnp.bfloat16)
        routes = product(routes, pick).astype(jnp.int32)
        expert = iota((EXPERTS, 1), 0)
        named = [expert == routes[k : k + 1] for k in range(TOPK)]
        earlier = iota((rows, 1), 0)
        before = (earlier // share == block) & (earlier < token)
        counts = product(select_matrix(named[0] | named[1]), select_matrix(before))
        slots = iota((EXPERTS * CAP * zs, 1), 0)
        inside = []
        for k in range(TOPK):
            ranks = jnp.sum(jnp.where(named[k], counts, 0.0), axis=0, keepdims=True)
            ranks = ranks.astype(jnp.int32)
            ranks_ref[k : k + 1, :] = ranks
            inside.append(slots == (routes[k : k + 1] * CAP + ranks) * zs + block)
        select_ref[...] = select_matrix(inside[0] | inside[1])

    depth = placed_ref.shape[1]
    columns = pl.ds(pl.multiple_of(step * depth, depth), depth)
    placed_ref[...] = product(select_ref[...], normed_ref[:, columns]).astype(jnp.bfloat16)


def prepare(place, tokens, gain, routes, zs):
    rows, width = tokens.shape
    half = rows // 2
    depth = 1024
    placed = EXPERTS * CAP * zs
    fixed = lambda i, p: (0, 0)
    return pl.pallas_call(
        functools.partial(prep_kernel, zs),
        grid_spec=pltpu.PrefetchScalarGridSpec(
            num_scalar_prefetch=1,
            grid=(width // depth,),
            in_specs=[
                pl.BlockSpec((zs, 1, MOE_SHARE, width), lambda i, p: (0, p[0], 0, 0)),
                pl.BlockSpec((1, width), fixed),
                pl.BlockSpec((TOPK, rows), fixed),
            ],
            out_specs=[
                pl.BlockSpec((placed, depth), lambda i, p: (0, i)),
                pl.BlockSpec((MOE_SHARE, width), fixed),
                pl.BlockSpec((TOPK, half), fixed),
            ],
            scratch_shapes=[
                pltpu.VMEM((half, width), jnp.bfloat16),
                pltpu.VMEM((placed, half), jnp.bfloat16),
            ],
        ),
        out_shape=[
            jax.ShapeDtypeStruct((placed, width), jnp.bfloat16),
            jax.ShapeDtypeStruct((MOE_SHARE, width), jnp.bfloat16),
            jax.ShapeDtypeStruct((TOPK, half), jnp.int32),
        ],
        cost_estimate=pl.CostEstimate(
            flops=2 * placed * half * width,
            bytes_accessed=2 * width * (half + placed),
            transcendentals=0,
        ),
        name="prepare",
    )(
        place,
        tokens.reshape(zs, 2, MOE_SHARE, width),
        gain.reshape(1, width),
        routes.T,
    )


def mixer_kernel(
    steps, place_ref, tokens_ref, halo_ref, before_ref, gain_ref, taps_mine, taps_theirs, *refs
):
    weights, (m0, m1), outs = refs[:6], refs[6:8], refs[8:-3]
    normed_ref, sums_ref, channels_ref = refs[-3:]
    step = pl.program_id(0)
    rows = channels_ref.shape[0]
    depth, half = weights[0].shape
    width = tokens_ref.shape[-1]
    blocks, _, tail_rows, _ = halo_ref.shape
    halos = blocks * tail_rows
    total = normed_ref.shape[0]
    reach = TAPS - 1

    @pl.when(step == 0)
    def _():
        gain = gain_ref[...]
        normed_ref[0:rows, :] = scaled_rows(tokens_ref[...].reshape(rows, width), gain)
        normed_ref[rows : rows + halos, :] = scaled_rows(halo_ref[...].reshape(halos, width), gain)
        normed_ref[rows + halos :, :] = scaled_rows(before_ref[...], gain)
        sums_ref[...] = jnp.zeros_like(sums_ref)

    @pl.when(step < steps)
    def _():
        piece = normed_ref[:, pl.ds(pl.multiple_of(step * depth, depth), depth)]
        joint = jnp.concatenate([weight[...] for weight in weights], axis=1)
        sums_ref[...] += product(piece, joint)

    @pl.when(step == steps - 1)
    def _():
        def pair(index):
            return sums_ref[:, 2 * index * half : 2 * (index + 1) * half]

        gated = (pair(1) * pair(0)).astype(jnp.bfloat16)
        row, source = iota((rows, 1), 0), iota((1, total), 1)
        place = row % MOE_SHARE
        ahead = row // MOE_SHARE + place_ref[0]
        tail = jnp.where(ahead == 0, total, rows + ahead * tail_rows)
        taps = jnp.concatenate([taps_mine[...], taps_theirs[...]], axis=1)
        mixed = None
        for tap in range(TAPS):
            back = reach - tap
            wanted = jnp.where(place >= back, row, tail + place) - back
            shifted = product(select_matrix(source == wanted), gated)
            term = taps[tap : tap + 1] * shifted
            mixed = term if mixed is None else mixed + term
        channels = (pair(2)[0:rows] * mixed).astype(jnp.bfloat16)
        target, source = iota((rows, 1), 0), iota((1, rows), 1)
        turned = (source // MOE_SHARE - place_ref[1] + blocks) % blocks
        order = select_matrix(target == turned * MOE_SHARE + source % MOE_SHARE)
        channels_ref[...] = product(order, channels).astype(jnp.bfloat16)

    write_chains(step - steps, MOE_SHARE, outs, lambda: product(
        channels_ref[...], jnp.concatenate([m0[...], m1[...]], axis=0)
    ))


def write_chains(step, rows, outs, compute):
    chains = len(outs) // 2
    pieces = chains * outs[0].shape[1] // 1024
    for piece in range(pieces):
        chain = piece * chains // pieces
        whole, sent = outs[chain], outs[chains + chain]
        start = (piece * 1024) % whole.shape[1]
        first = whole.shape[0] - rows if chain % 2 == 0 else rows

        @pl.when(step == piece)
        def _():
            total = compute().astype(jnp.bfloat16)
            whole[:, start : start + 1024] = total
            sent[:, start : start + 1024] = total[first : first + rows]


def chain_outputs(count, rows, width, chains):
    shapes = [(count, width // chains)] * chains + [(rows, width // chains)] * chains
    return (
        [pl.BlockSpec(shape, lambda *_: (0, 0)) for shape in shapes],
        [jax.ShapeDtypeStruct(shape, jnp.bfloat16) for shape in shapes],
    )


def ring_sum(outs):
    chains = len(outs) // 2
    one = lax.optimization_barrier(jnp.ones((), jnp.bfloat16))
    wholes = [lax.optimization_barrier(whole * one) for whole in outs[:chains]]
    sums = list(outs[chains:])
    rows = sums[0].shape[0]
    zs = lax.axis_size("z")
    for hop in range(zs - 1):
        for chain in range(chains):
            way = 1 if chain % 2 == 0 else -1
            came = lax.ppermute(sums[chain], "z", [(i, (i + way) % zs) for i in range(zs)])
            block = (zs - 2 - hop) if way == 1 else (hop + 2) % zs
            mine = wholes[chain][block * rows : (block + 1) * rows]
            total = came.astype(jnp.float32) + mine.astype(jnp.float32)
            sums[chain] = total.astype(jnp.bfloat16)
    return sums


def mixer_partial(place, tokens, before, gain, taps, weights, mixes, zs):
    rows, width = tokens.shape
    half = rows // 2
    channels = weights[0].shape[1]
    depth = 1024
    steps = width // depth
    tail_rows = MOE_SHARE // 2
    total = half + zs * tail_rows + before.shape[0]
    fixed = lambda i, c: (0, 0)
    after = lambda i, c: (0, jnp.maximum(i - steps, 0))
    out_specs, out_shape = chain_outputs(half, MOE_SHARE, width, MIX_CHAINS)
    split = tokens.reshape(zs, 2, MOE_SHARE, width)
    return pl.pallas_call(
        functools.partial(mixer_kernel, steps),
        grid_spec=pltpu.PrefetchScalarGridSpec(
            num_scalar_prefetch=1,
            grid=(2 * steps,),
            in_specs=[
                pl.BlockSpec((zs, 1, MOE_SHARE, width), lambda i, c: (0, c[0], 0, 0)),
                pl.BlockSpec((zs, 1, tail_rows, width), lambda i, c: (0, 1 - c[0], 1, 0)),
                pl.BlockSpec(before.shape, fixed),
                pl.BlockSpec((1, width), fixed),
                pl.BlockSpec((TAPS, channels), fixed),
                pl.BlockSpec((TAPS, channels), fixed),
            ]
            + [pl.BlockSpec((depth, channels), lambda i, c: (jnp.minimum(i, steps - 1), 0))] * 6
            + [pl.BlockSpec((channels, depth), after)] * 2,
            out_specs=out_specs,
            scratch_shapes=[
                pltpu.VMEM((total, width), jnp.bfloat16),
                pltpu.VMEM((total, 6 * channels), jnp.float32),
                pltpu.VMEM((half, 2 * channels), jnp.bfloat16),
            ],
        ),
        out_shape=out_shape,
        cost_estimate=pl.CostEstimate(
            flops=2 * width * channels * (6 * total + 2 * half),
            bytes_accessed=2 * width * (total + half + 8 * channels),
            transcendentals=0,
        ),
        name="mixer",
    )(place, split, split, before, gain.reshape(1, width), *taps, *weights, *mixes)


def expert_kernel(zs, steps, rows_ref, g0, g1, u0, u1, d0, d1, out_ref, sums_ref, units_ref):
    step = pl.program_id(0)
    count = rows_ref.shape[0]
    units = 2 * g0.shape[1]

    @pl.when(step == 0)
    def _():
        sums_ref[...] = jnp.zeros_like(sums_ref)

    @pl.when(step < steps)
    def _():
        joint = jnp.concatenate([g0[...], g1[...], u0[...], u1[...]], axis=1)
        sums_ref[...] += product(rows_ref[...], joint)

    @pl.when(step == steps - 1)
    def _():
        target, source = iota((count, 1), 0), iota((1, count), 1)
        order = select_matrix(target == (source % zs) * (count // zs) + source // zs)
        gate, up = sums_ref[:, :units], sums_ref[:, units:]
        hidden = (gate * jax.nn.sigmoid(gate) * up).astype(jnp.bfloat16)
        units_ref[...] = product(order, hidden).astype(jnp.bfloat16)

    @pl.when(step >= steps)
    def _():
        joint = jnp.concatenate([d0[...], d1[...]], axis=0)
        out_ref[...] = product(units_ref[...], joint).astype(jnp.bfloat16)


def expert_partial(rows, weights, downs, zs):
    count, width = rows.shape
    half = weights[0].shape[1]
    depth = 1024
    steps = width // depth
    early = lambda i: jnp.minimum(i, steps - 1)
    after = lambda i: jnp.maximum(i - steps, 0)
    return pl.pallas_call(
        functools.partial(expert_kernel, zs, steps),
        grid=(2 * steps,),
        in_specs=[pl.BlockSpec((count, depth), lambda i: (0, early(i)))]
        + [pl.BlockSpec((depth, half), lambda i: (early(i), 0))] * 4
        + [pl.BlockSpec((half, depth), lambda i: (0, after(i)))] * 2,
        out_specs=pl.BlockSpec((count, depth), lambda i: (0, after(i))),
        scratch_shapes=[
            pltpu.VMEM((count, 4 * half), jnp.float32),
            pltpu.VMEM((count, 2 * half), jnp.bfloat16),
        ],
        out_shape=jax.ShapeDtypeStruct((count, width), jnp.bfloat16),
        cost_estimate=pl.CostEstimate(
            flops=12 * width * half * count,
            bytes_accessed=2 * width * (2 * count + 6 * half),
            transcendentals=2 * count * half,
        ),
        name="experts",
    )(rows, *weights, *downs)


def layer(
    mix_tokens,
    mix_gain,
    value_weight,
    inner_weight,
    outer_weight,
    conv_taps,
    mix_weight,
    moe_tokens,
    moe_gain,
    router_group,
    router_expert,
    expert_routes,
    gate_weight,
    up_weight,
    down_weight,
):
    z_index = lax.axis_index("z")
    core = lax.axis_index("core")
    zs = lax.axis_size("z")
    eps = lax.axis_size(EP)
    width = moe_tokens.shape[1]
    core_ref = jnp.stack([core, z_index]).astype(jnp.int32)

    gate, up, down = gate_weight[0], up_weight[0], down_weight[0]
    theirs = [swap_cores(array) for array in (gate, up, down)]

    placed, own_normed, half_ranks = prepare(
        core_ref, moe_tokens, moe_gain, expert_routes, zs
    )
    placed, own_normed, half_ranks, theirs = lax.optimization_barrier(
        (placed, own_normed, half_ranks, theirs)
    )

    def exchange(array):
        return lax.all_to_all(array, EP, split_axis=0, concat_axis=0, tiled=True)

    arrived = exchange(placed.reshape(EXPERTS, CAP * zs, width)).reshape(-1, width)
    partial_value = expert_partial(arrived, (gate, theirs[0], up, theirs[1]), (down, theirs[2]), zs)
    summed = lax.psum_scatter(partial_value, "z", scatter_dimension=0, tiled=True)

    _, later = lax.optimization_barrier(
        (
            partial_value,
            (
                mix_tokens,
                (value_weight, inner_weight, outer_weight),
                (conv_taps, mix_weight),
                own_normed,
                half_ranks,
                expert_routes,
            ),
        )
    )
    mix_tokens, projections, (conv_taps, mix_weight), own_normed, half_ranks, expert_routes = later
    before = lax.ppermute(
        mix_tokens[mix_tokens.shape[0] - MOE_SHARE :], EP, [(i, i + 1) for i in range(eps - 1)]
    )
    taps = (conv_taps, swap_late(conv_taps))
    weights = [part for array in projections for part in (array, swap_late(array))]
    mixes = (mix_weight, swap_late(mix_weight))
    partial_mix = mixer_partial(core_ref, mix_tokens, before, mix_gain, taps, weights, mixes, zs)
    mixer_sums = ring_sum(partial_mix)
    summed, mixer_sums = lax.optimization_barrier((summed, mixer_sums))
    mixer_out = jnp.concatenate(mixer_sums, axis=1)
    returned = exchange(summed.reshape(eps, CAP * width // 128, 128)).reshape(-1, width)

    own_routes = lax.dynamic_slice_in_dim(
        expert_routes, (2 * z_index + core) * MOE_SHARE, MOE_SHARE, 0
    )
    own_ranks = lax.dynamic_slice_in_dim(half_ranks, z_index * MOE_SHARE, MOE_SHARE, 1).T
    token_weights = route_weights(own_normed, own_routes, router_group, router_expert)

    position = own_routes * CAP + own_ranks
    targets = jnp.arange(EXPERTS * CAP, dtype=jnp.int32)
    spread = jnp.sum(
        jnp.where(position[:, :, None] == targets, token_weights[:, :, None], 0.0), axis=1
    )
    expert_out = jnp.dot(
        spread,
        returned.astype(jnp.float32),
        precision=lax.Precision.HIGHEST,
        preferred_element_type=jnp.float32,
    )
    return (mixer_out, expert_out.astype(jnp.bfloat16))


def solution(mesh):
    torus = Mesh(mesh.devices.reshape(4, 4, 8, 2), ALL)
    return jax.shard_map(
        layer,
        mesh=torus,
        in_specs=(
            P(EP, None),
            P(),
            P(None, TP),
            P(None, TP),
            P(None, TP),
            P(None, TP),
            P(TP, None),
            P(EP, None),
            P(),
            P(),
            P(),
            P(EP, None),
            P(EP, None, TP),
            P(EP, None, TP),
            P(EP, TP, None),
        ),
        out_specs=(P(ALL, None), P(ALL, None)),
        check_vma=False,
    )
```

```python
import functools

import jax
import jax.numpy as jnp
from jax import lax
from jax.experimental import pallas as pl
from jax.experimental.pallas import tpu as pltpu
from jax.sharding import Mesh
from jax.sharding import PartitionSpec as P


TAPS = 3
EXPERTS = 16
GROUPS = 4
TOPK = 2
MOE_SHARE = 16
EPG = 4
CAP = 4


MIX_CHAINS = 2

EP = ("y", "x")
TP = ("z", "core")
ALL = EP + TP


def route_weights(normed, routes, router_group, router_expert):
    group_logit = jnp.dot(normed, router_group, preferred_element_type=jnp.float32)
    expert_logit = jnp.dot(normed, router_expert, preferred_element_type=jnp.float32)
    group_exp = jnp.exp(group_logit)
    group_id = routes[:, 0] // EPG
    group_pick = (group_id[:, None] == jnp.arange(GROUPS, dtype=jnp.int32)[None, :]).astype(
        jnp.float32
    )
    group_gate = jnp.sum(group_exp * group_pick, axis=1) / jnp.sum(group_exp, axis=1)
    expert_pick = (
        routes[:, :, None] == jnp.arange(EXPERTS, dtype=jnp.int32)[None, None, :]
    ).astype(jnp.float32)
    chosen = jnp.exp(jnp.sum(expert_logit[:, None, :] * expert_pick, axis=2))
    return group_gate[:, None] * chosen / jnp.sum(chosen, axis=1, keepdims=True)


def swap_cores(value):
    return lax.ppermute(value, "core", [(0, 1), (1, 0)])


def swap_late(value):
    return lax.ppermute(value, "core", [(0, 1), (1, 0)])


def iota(shape, dim):
    return lax.broadcasted_iota(jnp.int32, shape, dim)


def select_matrix(mask):
    return jnp.where(mask, 1.0, 0.0).astype(jnp.bfloat16)


def product(left, right):
    return jnp.dot(left, right, preferred_element_type=jnp.float32)


def scaled_rows(rows, gain):
    values = rows.astype(jnp.float32)
    inverse = lax.rsqrt(jnp.mean(values * values, axis=-1, keepdims=True) + 1e-06)
    return (values * inverse * gain).astype(jnp.bfloat16)


def prep_kernel(
    zs, place_ref, tokens_ref, gain_ref, routes_ref, placed_ref, own_ref, ranks_ref,
    normed_ref, select_ref
):
    share = MOE_SHARE
    rows = zs * share
    width = tokens_ref.shape[-1]
    step = pl.program_id(0)

    @pl.when(step == 0)
    def _():
        normed_ref[...] = scaled_rows(tokens_ref[...].reshape(rows, width), gain_ref[...])
        own_ref[...] = normed_ref[pl.ds(pl.multiple_of(place_ref[1] * share, share), share), :]
        token = iota((1, rows), 1)
        block = token // share
        source = block * (2 * share) + place_ref[0] * share + token % share
        pick = select_matrix(iota((2 * rows, 1), 0) == source)
        routes = routes_ref[...].astype(jnp.float32).astype(jnp.bfloat16)
        routes = product(routes, pick).astype(jnp.int32)
        expert = iota((EXPERTS, 1), 0)
        named = [expert == routes[k : k + 1] for k in range(TOPK)]
        earlier = iota((rows, 1), 0)
        before = (earlier // share == block) & (earlier < token)
        counts = product(select_matrix(named[0] | named[1]), select_matrix(before))
        slots = iota((EXPERTS * CAP * zs, 1), 0)
        inside = []
        for k in range(TOPK):
            ranks = jnp.sum(jnp.where(named[k], counts, 0.0), axis=0, keepdims=True)
            ranks = ranks.astype(jnp.int32)
            ranks_ref[k : k + 1, :] = ranks
            inside.append(slots == (routes[k : k + 1] * CAP + ranks) * zs + block)
        select_ref[...] = select_matrix(inside[0] | inside[1])

    depth = placed_ref.shape[1]
    columns = pl.ds(pl.multiple_of(step * depth, depth), depth)
    placed_ref[...] = product(select_ref[...], normed_ref[:, columns]).astype(jnp.bfloat16)


def prepare(place, tokens, gain, routes, zs):
    rows, width = tokens.shape
    half = rows // 2
    depth = 2048
    placed = EXPERTS * CAP * zs
    fixed = lambda i, p: (0, 0)
    return pl.pallas_call(
        functools.partial(prep_kernel, zs),
        grid_spec=pltpu.PrefetchScalarGridSpec(
            num_scalar_prefetch=1,
            grid=(width // depth,),
            in_specs=[
                pl.BlockSpec((zs, 1, MOE_SHARE, width), lambda i, p: (0, p[0], 0, 0)),
                pl.BlockSpec((1, width), fixed),
                pl.BlockSpec((TOPK, rows), fixed),
            ],
            out_specs=[
                pl.BlockSpec((placed, depth), lambda i, p: (0, i)),
                pl.BlockSpec((MOE_SHARE, width), fixed),
                pl.BlockSpec((TOPK, half), fixed),
            ],
            scratch_shapes=[
                pltpu.VMEM((half, width), jnp.bfloat16),
                pltpu.VMEM((placed, half), jnp.bfloat16),
            ],
        ),
        out_shape=[
            jax.ShapeDtypeStruct((placed, width), jnp.bfloat16),
            jax.ShapeDtypeStruct((MOE_SHARE, width), jnp.bfloat16),
            jax.ShapeDtypeStruct((TOPK, half), jnp.int32),
        ],
        cost_estimate=pl.CostEstimate(
            flops=2 * placed * half * width,
            bytes_accessed=2 * width * (half + placed),
            transcendentals=0,
        ),
        name="prepare",
    )(
        place,
        tokens.reshape(zs, 2, MOE_SHARE, width),
        gain.reshape(1, width),
        routes.T,
    )


def mixer_kernel(
    steps, place_ref, tokens_ref, halo_ref, before_ref, gain_ref, taps_mine, taps_theirs, *refs
):
    weights, (m0, m1), outs = refs[:6], refs[6:8], refs[8:-3]
    normed_ref, sums_ref, channels_ref = refs[-3:]
    step = pl.program_id(0)
    rows = channels_ref.shape[0]
    depth, half = weights[0].shape
    width = tokens_ref.shape[-1]
    blocks, _, tail_rows, _ = halo_ref.shape
    halos = blocks * tail_rows
    total = normed_ref.shape[0]
    reach = TAPS - 1

    @pl.when(step == 0)
    def _():
        gain = gain_ref[...]
        normed_ref[0:rows, :] = scaled_rows(tokens_ref[...].reshape(rows, width), gain)
        normed_ref[rows : rows + halos, :] = scaled_rows(halo_ref[...].reshape(halos, width), gain)
        normed_ref[rows + halos :, :] = scaled_rows(before_ref[...], gain)
        sums_ref[...] = jnp.zeros_like(sums_ref)

    @pl.when(step < steps)
    def _():
        piece = normed_ref[:, pl.ds(pl.multiple_of(step * depth, depth), depth)]
        joint = jnp.concatenate([weight[...] for weight in weights], axis=1)
        sums_ref[...] += product(piece, joint)

    @pl.when(step == steps - 1)
    def _():
        def pair(index):
            return sums_ref[:, 2 * index * half : 2 * (index + 1) * half]

        gated = (pair(1) * pair(0)).astype(jnp.bfloat16)
        row, source = iota((rows, 1), 0), iota((1, total), 1)
        place = row % MOE_SHARE
        ahead = row // MOE_SHARE + place_ref[0]
        tail = jnp.where(ahead == 0, total, rows + ahead * tail_rows)
        taps = jnp.concatenate([taps_mine[...], taps_theirs[...]], axis=1)
        mixed = None
        for tap in range(TAPS):
            back = reach - tap
            wanted = jnp.where(place >= back, row, tail + place) - back
            shifted = product(select_matrix(source == wanted), gated)
            term = taps[tap : tap + 1] * shifted
            mixed = term if mixed is None else mixed + term
        channels = (pair(2)[0:rows] * mixed).astype(jnp.bfloat16)
        target, source = iota((rows, 1), 0), iota((1, rows), 1)
        turned = (source // MOE_SHARE - place_ref[1] + blocks) % blocks
        order = select_matrix(target == turned * MOE_SHARE + source % MOE_SHARE)
        channels_ref[...] = product(order, channels).astype(jnp.bfloat16)

    write_chains(step - steps, MOE_SHARE, outs, lambda: product(
        channels_ref[...], jnp.concatenate([m0[...], m1[...]], axis=0)
    ))


def write_chains(step, rows, outs, compute):
    chains = len(outs) // 2
    pieces = chains * outs[0].shape[1] // 1024
    for piece in range(pieces):
        chain = piece * chains // pieces
        whole, sent = outs[chain], outs[chains + chain]
        start = (piece * 1024) % whole.shape[1]
        first = whole.shape[0] - rows if chain % 2 == 0 else rows

        @pl.when(step == piece)
        def _():
            total = compute().astype(jnp.bfloat16)
            whole[:, start : start + 1024] = total
            sent[:, start : start + 1024] = total[first : first + rows]


def chain_outputs(count, rows, width, chains):
    shapes = [(count, width // chains)] * chains + [(rows, width // chains)] * chains
    return (
        [pl.BlockSpec(shape, lambda *_: (0, 0)) for shape in shapes],
        [jax.ShapeDtypeStruct(shape, jnp.bfloat16) for shape in shapes],
    )


def ring_sum(outs):
    chains = len(outs) // 2
    one = lax.optimization_barrier(jnp.ones((), jnp.bfloat16))
    wholes = [lax.optimization_barrier(whole * one) for whole in outs[:chains]]
    sums = list(outs[chains:])
    rows = sums[0].shape[0]
    zs = lax.axis_size("z")
    held = sums
    for hop in range(zs - 1):
        if hop == zs - 2:
            held = list(sums)
        for chain in range(chains):
            way = 1 if chain % 2 == 0 else -1
            came = lax.ppermute(sums[chain], "z", [(i, (i + way) % zs) for i in range(zs)])
            block = (zs - 2 - hop) if way == 1 else (hop + 2) % zs
            mine = wholes[chain][block * rows : (block + 1) * rows]
            total = came.astype(jnp.float32) + mine.astype(jnp.float32)
            sums[chain] = total.astype(jnp.bfloat16)
    return sums, held


def mixer_partial(place, tokens, before, gain, taps, weights, mixes, zs):
    rows, width = tokens.shape
    half = rows // 2
    channels = weights[0].shape[1]
    depth = 1024
    steps = width // depth
    tail_rows = MOE_SHARE // 2
    total = half + zs * tail_rows + before.shape[0]
    fixed = lambda i, c: (0, 0)
    after = lambda i, c: (0, jnp.maximum(i - steps, 0))
    out_specs, out_shape = chain_outputs(half, MOE_SHARE, width, MIX_CHAINS)
    split = tokens.reshape(zs, 2, MOE_SHARE, width)
    return pl.pallas_call(
        functools.partial(mixer_kernel, steps),
        grid_spec=pltpu.PrefetchScalarGridSpec(
            num_scalar_prefetch=1,
            grid=(2 * steps,),
            in_specs=[
                pl.BlockSpec((zs, 1, MOE_SHARE, width), lambda i, c: (0, c[0], 0, 0)),
                pl.BlockSpec((zs, 1, tail_rows, width), lambda i, c: (0, 1 - c[0], 1, 0)),
                pl.BlockSpec(before.shape, fixed),
                pl.BlockSpec((1, width), fixed),
                pl.BlockSpec((TAPS, channels), fixed),
                pl.BlockSpec((TAPS, channels), fixed),
            ]
            + [pl.BlockSpec((depth, channels), lambda i, c: (jnp.minimum(i, steps - 1), 0))] * 6
            + [pl.BlockSpec((channels, depth), after)] * 2,
            out_specs=out_specs,
            scratch_shapes=[
                pltpu.VMEM((total, width), jnp.bfloat16),
                pltpu.VMEM((total, 6 * channels), jnp.float32),
                pltpu.VMEM((half, 2 * channels), jnp.bfloat16),
            ],
        ),
        out_shape=out_shape,
        cost_estimate=pl.CostEstimate(
            flops=2 * width * channels * (6 * total + 2 * half),
            bytes_accessed=2 * width * (total + half + 8 * channels),
            transcendentals=0,
        ),
        name="mixer",
    )(place, split, split, before, gain.reshape(1, width), *taps, *weights, *mixes)


def expert_kernel(zs, steps, rows_ref, g0, g1, u0, u1, d0, d1, out_ref, sums_ref, units_ref):
    step = pl.program_id(0)
    count = rows_ref.shape[0]
    units = 2 * g0.shape[1]

    @pl.when(step == 0)
    def _():
        sums_ref[...] = jnp.zeros_like(sums_ref)

    @pl.when(step < steps)
    def _():
        joint = jnp.concatenate([g0[...], g1[...], u0[...], u1[...]], axis=1)
        sums_ref[...] += product(rows_ref[...], joint)

    @pl.when(step == steps - 1)
    def _():
        target, source = iota((count, 1), 0), iota((1, count), 1)
        order = select_matrix(target == (source % zs) * (count // zs) + source // zs)
        gate, up = sums_ref[:, :units], sums_ref[:, units:]
        hidden = (gate * jax.nn.sigmoid(gate) * up).astype(jnp.bfloat16)
        units_ref[...] = product(order, hidden).astype(jnp.bfloat16)

    @pl.when(step >= steps)
    def _():
        joint = jnp.concatenate([d0[...], d1[...]], axis=0)
        out_ref[...] = product(units_ref[...], joint).astype(jnp.bfloat16)


def expert_partial(rows, weights, downs, zs):
    count, width = rows.shape
    half = weights[0].shape[1]
    depth = 2048
    steps = width // depth
    early = lambda i: jnp.minimum(i, steps - 1)
    after = lambda i: jnp.maximum(i - steps, 0)
    return pl.pallas_call(
        functools.partial(expert_kernel, zs, steps),
        grid=(2 * steps,),
        in_specs=[pl.BlockSpec((count, depth), lambda i: (0, early(i)))]
        + [pl.BlockSpec((depth, half), lambda i: (early(i), 0))] * 4
        + [pl.BlockSpec((half, depth), lambda i: (0, after(i)))] * 2,
        out_specs=pl.BlockSpec((count, depth), lambda i: (0, after(i))),
        scratch_shapes=[
            pltpu.VMEM((count, 4 * half), jnp.float32),
            pltpu.VMEM((count, 2 * half), jnp.bfloat16),
        ],
        out_shape=jax.ShapeDtypeStruct((count, width), jnp.bfloat16),
        cost_estimate=pl.CostEstimate(
            flops=12 * width * half * count,
            bytes_accessed=2 * width * (2 * count + 6 * half),
            transcendentals=2 * count * half,
        ),
        name="experts",
    )(rows, *weights, *downs)


def layer(
    mix_tokens,
    mix_gain,
    value_weight,
    inner_weight,
    outer_weight,
    conv_taps,
    mix_weight,
    moe_tokens,
    moe_gain,
    router_group,
    router_expert,
    expert_routes,
    gate_weight,
    up_weight,
    down_weight,
):
    z_index = lax.axis_index("z")
    core = lax.axis_index("core")
    zs = lax.axis_size("z")
    eps = lax.axis_size(EP)
    width = moe_tokens.shape[1]
    core_ref = jnp.stack([core, z_index]).astype(jnp.int32)

    gate, up, down = gate_weight[0], up_weight[0], down_weight[0]
    theirs = [swap_cores(array) for array in (gate, up, down)]

    placed, own_normed, half_ranks = prepare(
        core_ref, moe_tokens, moe_gain, expert_routes, zs
    )
    placed, own_normed, half_ranks, theirs = lax.optimization_barrier(
        (placed, own_normed, half_ranks, theirs)
    )

    def exchange(array):
        return lax.all_to_all(array, EP, split_axis=0, concat_axis=0, tiled=True)

    arrived = exchange(placed.reshape(EXPERTS, CAP * zs, width)).reshape(-1, width)
    partial_value = expert_partial(arrived, (gate, theirs[0], up, theirs[1]), (down, theirs[2]), zs)
    summed = lax.psum_scatter(partial_value, "z", scatter_dimension=0, tiled=True)

    _, later = lax.optimization_barrier(
        (
            partial_value,
            (
                mix_tokens,
                (value_weight, inner_weight, outer_weight),
                (conv_taps, mix_weight),
                own_normed,
                half_ranks,
                expert_routes,
            ),
        )
    )
    mix_tokens, projections, (conv_taps, mix_weight), own_normed, half_ranks, expert_routes = later
    before = lax.ppermute(
        mix_tokens[mix_tokens.shape[0] - MOE_SHARE :], EP, [(i, i + 1) for i in range(eps - 1)]
    )
    taps = (conv_taps, swap_late(conv_taps))
    weights = [part for array in projections for part in (array, swap_late(array))]
    mixes = (mix_weight, swap_late(mix_weight))
    partial_mix = mixer_partial(core_ref, mix_tokens, before, mix_gain, taps, weights, mixes, zs)
    _, (own_normed, half_ranks, expert_routes) = lax.optimization_barrier(
        (partial_mix, (own_normed, half_ranks, expert_routes))
    )
    mixer_sums, held = ring_sum(partial_mix)
    mixer_out = jnp.concatenate(mixer_sums, axis=1)
    summed, _ = lax.optimization_barrier((summed, held))
    returned = exchange(summed.reshape(eps, CAP * width // 128, 128)).reshape(-1, width)

    own_routes = lax.dynamic_slice_in_dim(
        expert_routes, (2 * z_index + core) * MOE_SHARE, MOE_SHARE, 0
    )
    own_ranks = lax.dynamic_slice_in_dim(half_ranks, z_index * MOE_SHARE, MOE_SHARE, 1).T
    token_weights = route_weights(own_normed, own_routes, router_group, router_expert)

    position = own_routes * CAP + own_ranks
    targets = jnp.arange(EXPERTS * CAP, dtype=jnp.int32)
    spread = jnp.sum(
        jnp.where(position[:, :, None] == targets, token_weights[:, :, None], 0.0), axis=1
    )
    expert_out = jnp.dot(
        spread,
        returned.astype(jnp.float32),
        precision=lax.Precision.HIGHEST,
        preferred_element_type=jnp.float32,
    )
    return (mixer_out, expert_out.astype(jnp.bfloat16))


def solution(mesh):
    torus = Mesh(mesh.devices.reshape(4, 4, 8, 2), ALL)
    return jax.shard_map(
        layer,
        mesh=torus,
        in_specs=(
            P(EP, None),
            P(),
            P(None, TP),
            P(None, TP),
            P(None, TP),
            P(None, TP),
            P(TP, None),
            P(EP, None),
            P(),
            P(),
            P(),
            P(EP, None),
            P(EP, None, TP),
            P(EP, None, TP),
            P(EP, TP, None),
        ),
        out_specs=(P(ALL, None), P(ALL, None)),
        check_vma=False,
    )
```

```python
import functools

import jax
import jax.numpy as jnp
from jax import lax
from jax.experimental import pallas as pl
from jax.experimental.pallas import tpu as pltpu
from jax.sharding import Mesh
from jax.sharding import PartitionSpec as P


TAPS = 3
EXPERTS = 16
GROUPS = 4
TOPK = 2
MOE_SHARE = 16
EPG = 4
CAP = 4


MIX_CHAINS = 2

EP = ("y", "x")
TP = ("z", "core")
ALL = EP + TP


def route_weights(normed, routes, router_group, router_expert):
    group_logit = jnp.dot(normed, router_group, preferred_element_type=jnp.float32)
    expert_logit = jnp.dot(normed, router_expert, preferred_element_type=jnp.float32)
    group_exp = jnp.exp(group_logit)
    group_id = routes[:, 0] // EPG
    group_pick = (group_id[:, None] == jnp.arange(GROUPS, dtype=jnp.int32)[None, :]).astype(
        jnp.float32
    )
    group_gate = jnp.sum(group_exp * group_pick, axis=1) / jnp.sum(group_exp, axis=1)
    expert_pick = (
        routes[:, :, None] == jnp.arange(EXPERTS, dtype=jnp.int32)[None, None, :]
    ).astype(jnp.float32)
    chosen = jnp.exp(jnp.sum(expert_logit[:, None, :] * expert_pick, axis=2))
    return group_gate[:, None] * chosen / jnp.sum(chosen, axis=1, keepdims=True)


def swap_cores(value):
    return lax.ppermute(value, "core", [(0, 1), (1, 0)])


def swap_late(value):
    return lax.ppermute(value, "core", [(0, 1), (1, 0)])


def iota(shape, dim):
    return lax.broadcasted_iota(jnp.int32, shape, dim)


def select_matrix(mask):
    return jnp.where(mask, 1.0, 0.0).astype(jnp.bfloat16)


def product(left, right):
    return jnp.dot(left, right, preferred_element_type=jnp.float32)


def scaled_rows(rows, gain):
    values = rows.astype(jnp.float32)
    inverse = lax.rsqrt(jnp.mean(values * values, axis=-1, keepdims=True) + 1e-06)
    return (values * inverse * gain).astype(jnp.bfloat16)


def prep_kernel(
    zs, place_ref, tokens_ref, gain_ref, routes_ref, placed_ref, own_ref, ranks_ref,
    normed_ref, select_ref
):
    share = MOE_SHARE
    rows = zs * share
    width = tokens_ref.shape[-1]
    step = pl.program_id(0)

    @pl.when(step == 0)
    def _():
        normed_ref[...] = scaled_rows(tokens_ref[...].reshape(rows, width), gain_ref[...])
        own_ref[...] = normed_ref[pl.ds(pl.multiple_of((place_ref[0] >> 1) * share, share), share), :]
        token = iota((1, rows), 1)
        block = token // share
        source = block * (2 * share) + (place_ref[0] & 1) * share + token % share
        pick = select_matrix(iota((2 * rows, 1), 0) == source)
        routes = routes_ref[...].astype(jnp.float32).astype(jnp.bfloat16)
        routes = product(routes, pick).astype(jnp.int32)
        expert = iota((EXPERTS, 1), 0)
        named = [expert == routes[k : k + 1] for k in range(TOPK)]
        earlier = iota((rows, 1), 0)
        before = (earlier // share == block) & (earlier < token)
        counts = product(select_matrix(named[0] | named[1]), select_matrix(before))
        slots = iota((EXPERTS * CAP * zs, 1), 0)
        inside = []
        for k in range(TOPK):
            ranks = jnp.sum(jnp.where(named[k], counts, 0.0), axis=0, keepdims=True)
            ranks = ranks.astype(jnp.int32)
            ranks_ref[k : k + 1, :] = ranks
            inside.append(slots == (routes[k : k + 1] * CAP + ranks) * zs + block)
        select_ref[...] = select_matrix(inside[0] | inside[1])

    depth = placed_ref.shape[1]
    columns = pl.ds(pl.multiple_of(step * depth, depth), depth)
    placed_ref[...] = product(select_ref[...], normed_ref[:, columns]).astype(jnp.bfloat16)


def prepare(place, tokens, gain, routes, zs):
    rows, width = tokens.shape
    half = rows // 2
    depth = 2048
    placed = EXPERTS * CAP * zs
    fixed = lambda i, p: (0, 0)
    return pl.pallas_call(
        functools.partial(prep_kernel, zs),
        grid_spec=pltpu.PrefetchScalarGridSpec(
            num_scalar_prefetch=1,
            grid=(width // depth,),
            in_specs=[
                pl.BlockSpec((zs, 1, MOE_SHARE, width), lambda i, p: (0, (p[0] & 1), 0, 0)),
                pl.BlockSpec((1, width), fixed),
                pl.BlockSpec((TOPK, rows), fixed),
            ],
            out_specs=[
                pl.BlockSpec((placed, depth), lambda i, p: (0, i)),
                pl.BlockSpec((MOE_SHARE, width), fixed),
                pl.BlockSpec((TOPK, half), fixed),
            ],
            scratch_shapes=[
                pltpu.VMEM((half, width), jnp.bfloat16),
                pltpu.VMEM((placed, half), jnp.bfloat16),
            ],
        ),
        out_shape=[
            jax.ShapeDtypeStruct((placed, width), jnp.bfloat16),
            jax.ShapeDtypeStruct((MOE_SHARE, width), jnp.bfloat16),
            jax.ShapeDtypeStruct((TOPK, half), jnp.int32),
        ],
        cost_estimate=pl.CostEstimate(
            flops=2 * placed * half * width,
            bytes_accessed=2 * width * (half + placed),
            transcendentals=0,
        ),
        name="prepare",
    )(
        place,
        tokens.reshape(zs, 2, MOE_SHARE, width),
        gain.reshape(1, width),
        routes.T,
    )


def mixer_kernel(
    steps, place_ref, tokens_ref, halo_ref, before_ref, gain_ref, taps_mine, taps_theirs, *refs
):
    weights, (m0, m1), outs = refs[:6], refs[6:8], refs[8:-3]
    normed_ref, sums_ref, channels_ref = refs[-3:]
    step = pl.program_id(0)
    rows = channels_ref.shape[0]
    depth, half = weights[0].shape
    width = tokens_ref.shape[-1]
    blocks, _, tail_rows, _ = halo_ref.shape
    halos = blocks * tail_rows
    total = normed_ref.shape[0]
    reach = TAPS - 1

    @pl.when(step == 0)
    def _():
        gain = gain_ref[...]
        normed_ref[0:rows, :] = scaled_rows(tokens_ref[...].reshape(rows, width), gain)
        normed_ref[rows : rows + halos, :] = scaled_rows(halo_ref[...].reshape(halos, width), gain)
        normed_ref[rows + halos :, :] = scaled_rows(before_ref[...], gain)
        sums_ref[...] = jnp.zeros_like(sums_ref)

    @pl.when(step < steps)
    def _():
        piece = normed_ref[:, pl.ds(pl.multiple_of(step * depth, depth), depth)]
        joint = jnp.concatenate([weight[...] for weight in weights], axis=1)
        sums_ref[...] += product(piece, joint)

    @pl.when(step == steps - 1)
    def _():
        def pair(index):
            return sums_ref[:, 2 * index * half : 2 * (index + 1) * half]

        gated = (pair(1) * pair(0)).astype(jnp.bfloat16)
        row, source = iota((rows, 1), 0), iota((1, total), 1)
        place = row % MOE_SHARE
        ahead = row // MOE_SHARE + (place_ref[0] & 1)
        tail = jnp.where(ahead == 0, total, rows + ahead * tail_rows)
        taps = jnp.concatenate([taps_mine[...], taps_theirs[...]], axis=1)
        mixed = None
        for tap in range(TAPS):
            back = reach - tap
            wanted = jnp.where(place >= back, row, tail + place) - back
            shifted = product(select_matrix(source == wanted), gated)
            term = taps[tap : tap + 1] * shifted
            mixed = term if mixed is None else mixed + term
        channels = (pair(2)[0:rows] * mixed).astype(jnp.bfloat16)
        target, source = iota((rows, 1), 0), iota((1, rows), 1)
        turned = (source // MOE_SHARE - (place_ref[0] >> 1) + blocks) % blocks
        order = select_matrix(target == turned * MOE_SHARE + source % MOE_SHARE)
        channels_ref[...] = product(order, channels).astype(jnp.bfloat16)

    write_chains(step - steps, MOE_SHARE, outs, lambda: product(
        channels_ref[...], jnp.concatenate([m0[...], m1[...]], axis=0)
    ))


def write_chains(step, rows, outs, compute):
    chains = len(outs) // 2
    pieces = chains * outs[0].shape[1] // 1024
    for piece in range(pieces):
        chain = piece * chains // pieces
        whole, sent = outs[chain], outs[chains + chain]
        start = (piece * 1024) % whole.shape[1]
        first = whole.shape[0] - rows if chain % 2 == 0 else rows

        @pl.when(step == piece)
        def _():
            total = compute().astype(jnp.bfloat16)
            whole[:, start : start + 1024] = total
            sent[:, start : start + 1024] = total[first : first + rows]


def chain_outputs(count, rows, width, chains):
    shapes = [(count, width // chains)] * chains + [(rows, width // chains)] * chains
    return (
        [pl.BlockSpec(shape, lambda *_: (0, 0)) for shape in shapes],
        [jax.ShapeDtypeStruct(shape, jnp.bfloat16) for shape in shapes],
    )


def ring_sum(outs):
    chains = len(outs) // 2
    one = lax.optimization_barrier(jnp.ones((), jnp.bfloat16))
    wholes = [lax.optimization_barrier(whole * one) for whole in outs[:chains]]
    sums = list(outs[chains:])
    rows = sums[0].shape[0]
    zs = lax.axis_size("z")
    held = sums
    for hop in range(zs - 1):
        if hop == zs - 2:
            held = list(sums)
        for chain in range(chains):
            way = 1 if chain % 2 == 0 else -1
            came = lax.ppermute(sums[chain], "z", [(i, (i + way) % zs) for i in range(zs)])
            block = (zs - 2 - hop) if way == 1 else (hop + 2) % zs
            mine = wholes[chain][block * rows : (block + 1) * rows]
            total = came.astype(jnp.float32) + mine.astype(jnp.float32)
            sums[chain] = total.astype(jnp.bfloat16)
    return sums, held


def mixer_partial(place, tokens, before, gain, taps, weights, mixes, zs):
    rows, width = tokens.shape
    half = rows // 2
    channels = weights[0].shape[1]
    depth = 1024
    steps = width // depth
    tail_rows = MOE_SHARE // 2
    total = half + zs * tail_rows + before.shape[0]
    fixed = lambda i, c: (0, 0)
    after = lambda i, c: (0, jnp.maximum(i - steps, 0))
    out_specs, out_shape = chain_outputs(half, MOE_SHARE, width, MIX_CHAINS)
    split = tokens.reshape(zs, 2, MOE_SHARE, width)
    return pl.pallas_call(
        functools.partial(mixer_kernel, steps),
        grid_spec=pltpu.PrefetchScalarGridSpec(
            num_scalar_prefetch=1,
            grid=(2 * steps,),
            in_specs=[
                pl.BlockSpec((zs, 1, MOE_SHARE, width), lambda i, c: (0, (c[0] & 1), 0, 0)),
                pl.BlockSpec((zs, 1, tail_rows, width), lambda i, c: (0, 1 - (c[0] & 1), 1, 0)),
                pl.BlockSpec(before.shape, fixed),
                pl.BlockSpec((1, width), fixed),
                pl.BlockSpec((TAPS, channels), fixed),
                pl.BlockSpec((TAPS, channels), fixed),
            ]
            + [pl.BlockSpec((depth, channels), lambda i, c: (jnp.minimum(i, steps - 1), 0))] * 6
            + [pl.BlockSpec((channels, depth), after)] * 2,
            out_specs=out_specs,
            scratch_shapes=[
                pltpu.VMEM((total, width), jnp.bfloat16),
                pltpu.VMEM((total, 6 * channels), jnp.float32),
                pltpu.VMEM((half, 2 * channels), jnp.bfloat16),
            ],
        ),
        out_shape=out_shape,
        cost_estimate=pl.CostEstimate(
            flops=2 * width * channels * (6 * total + 2 * half),
            bytes_accessed=2 * width * (total + half + 8 * channels),
            transcendentals=0,
        ),
        name="mixer",
    )(place, split, split, before, gain.reshape(1, width), *taps, *weights, *mixes)


def expert_kernel(zs, steps, rows_ref, g0, g1, u0, u1, d0, d1, out_ref, sums_ref, units_ref):
    step = pl.program_id(0)
    count = rows_ref.shape[0]
    units = 2 * g0.shape[1]

    @pl.when(step == 0)
    def _():
        sums_ref[...] = jnp.zeros_like(sums_ref)

    @pl.when(step < steps)
    def _():
        joint = jnp.concatenate([g0[...], g1[...], u0[...], u1[...]], axis=1)
        sums_ref[...] += product(rows_ref[...], joint)

    @pl.when(step == steps - 1)
    def _():
        target, source = iota((count, 1), 0), iota((1, count), 1)
        order = select_matrix(target == (source % zs) * (count // zs) + source // zs)
        gate, up = sums_ref[:, :units], sums_ref[:, units:]
        hidden = (gate * jax.nn.sigmoid(gate) * up).astype(jnp.bfloat16)
        units_ref[...] = product(order, hidden).astype(jnp.bfloat16)

    @pl.when(step >= steps)
    def _():
        joint = jnp.concatenate([d0[...], d1[...]], axis=0)
        out_ref[...] = product(units_ref[...], joint).astype(jnp.bfloat16)


def expert_partial(rows, weights, downs, zs):
    count, width = rows.shape
    half = weights[0].shape[1]
    depth = 2048
    steps = width // depth
    early = lambda i: jnp.minimum(i, steps - 1)
    after = lambda i: jnp.maximum(i - steps, 0)
    return pl.pallas_call(
        functools.partial(expert_kernel, zs, steps),
        grid=(2 * steps,),
        in_specs=[pl.BlockSpec((count, depth), lambda i: (0, early(i)))]
        + [pl.BlockSpec((depth, half), lambda i: (early(i), 0))] * 4
        + [pl.BlockSpec((half, depth), lambda i: (0, after(i)))] * 2,
        out_specs=pl.BlockSpec((count, depth), lambda i: (0, after(i))),
        scratch_shapes=[
            pltpu.VMEM((count, 4 * half), jnp.float32),
            pltpu.VMEM((count, 2 * half), jnp.bfloat16),
        ],
        out_shape=jax.ShapeDtypeStruct((count, width), jnp.bfloat16),
        cost_estimate=pl.CostEstimate(
            flops=12 * width * half * count,
            bytes_accessed=2 * width * (2 * count + 6 * half),
            transcendentals=2 * count * half,
        ),
        name="experts",
    )(rows, *weights, *downs)


def layer(
    mix_tokens,
    mix_gain,
    value_weight,
    inner_weight,
    outer_weight,
    conv_taps,
    mix_weight,
    moe_tokens,
    moe_gain,
    router_group,
    router_expert,
    expert_routes,
    gate_weight,
    up_weight,
    down_weight,
):
    z_index = lax.axis_index("z")
    core = lax.axis_index("core")
    zs = lax.axis_size("z")
    eps = lax.axis_size(EP)
    width = moe_tokens.shape[1]
    core_ref = (2 * z_index + core).reshape(1).astype(jnp.int32)

    gate, up, down = gate_weight[0], up_weight[0], down_weight[0]
    theirs = [swap_cores(array) for array in (gate, up, down)]

    placed, own_normed, half_ranks = prepare(
        core_ref, moe_tokens, moe_gain, expert_routes, zs
    )
    placed, own_normed, half_ranks, theirs = lax.optimization_barrier(
        (placed, own_normed, half_ranks, theirs)
    )

    def exchange(array):
        return lax.all_to_all(array, EP, split_axis=0, concat_axis=0, tiled=True)

    arrived = exchange(placed.reshape(EXPERTS, CAP * zs, width)).reshape(-1, width)
    partial_value = expert_partial(arrived, (gate, theirs[0], up, theirs[1]), (down, theirs[2]), zs)
    summed = lax.psum_scatter(partial_value, "z", scatter_dimension=0, tiled=True)

    _, later = lax.optimization_barrier(
        (
            partial_value,
            (
                mix_tokens,
                (value_weight, inner_weight, outer_weight),
                (conv_taps, mix_weight),
                own_normed,
                half_ranks,
                expert_routes,
            ),
        )
    )
    mix_tokens, projections, (conv_taps, mix_weight), own_normed, half_ranks, expert_routes = later
    before = lax.ppermute(
        mix_tokens[mix_tokens.shape[0] - MOE_SHARE :], EP, [(i, i + 1) for i in range(eps - 1)]
    )
    taps = (conv_taps, swap_late(conv_taps))
    weights = [part for array in projections for part in (array, swap_late(array))]
    mixes = (mix_weight, swap_late(mix_weight))
    partial_mix = mixer_partial(core_ref, mix_tokens, before, mix_gain, taps, weights, mixes, zs)
    _, (own_normed, half_ranks, expert_routes) = lax.optimization_barrier(
        (partial_mix, (own_normed, half_ranks, expert_routes))
    )
    mixer_sums, held = ring_sum(partial_mix)
    mixer_out = jnp.concatenate(mixer_sums, axis=1)
    summed, _ = lax.optimization_barrier((summed, held))
    returned = exchange(summed.reshape(eps, CAP * width // 128, 128)).reshape(-1, width)

    own_routes = lax.dynamic_slice_in_dim(
        expert_routes, (2 * z_index + core) * MOE_SHARE, MOE_SHARE, 0
    )
    own_ranks = lax.dynamic_slice_in_dim(half_ranks, z_index * MOE_SHARE, MOE_SHARE, 1).T
    token_weights = route_weights(own_normed, own_routes, router_group, router_expert)

    position = own_routes * CAP + own_ranks
    targets = jnp.arange(EXPERTS * CAP, dtype=jnp.int32)
    spread = jnp.sum(
        jnp.where(position[:, :, None] == targets, token_weights[:, :, None], 0.0), axis=1
    )
    expert_out = jnp.dot(
        spread,
        returned.astype(jnp.float32),
        precision=lax.Precision.HIGHEST,
        preferred_element_type=jnp.float32,
    )
    return (mixer_out, expert_out.astype(jnp.bfloat16))


def solution(mesh):
    torus = Mesh(mesh.devices.reshape(4, 4, 8, 2), ALL)
    return jax.shard_map(
        layer,
        mesh=torus,
        in_specs=(
            P(EP, None),
            P(),
            P(None, TP),
            P(None, TP),
            P(None, TP),
            P(None, TP),
            P(TP, None),
            P(EP, None),
            P(),
            P(),
            P(),
            P(EP, None),
            P(EP, None, TP),
            P(EP, None, TP),
            P(EP, TP, None),
        ),
        out_specs=(P(ALL, None), P(ALL, None)),
        check_vma=False,
    )
```
